512 devices in a mesh: sp: 64 (over z, y), tp: 4 (over x), dp: 2 (over core).
Axes of the slice: x: 4, y: 8, z: 8, core: 2. Of those that a mesh axis runs over, the one named last changes fastest.
Arguments:
- latent: bfloat16 [2, 8192, 2048], P('dp', ('sp', 'tp')), may hold values from -10 to 10
- condition: bfloat16 [2, 2048], P('dp'), may hold values from -6 to 6
- context: bfloat16 [2, 512, 2048], P('dp', 'sp'), may hold values from -6 to 6
- context_source: bfloat16 [2048], replicated, may hold values from -6 to 6
- mod_weight: bfloat16 [3, 2048, 2048], P(None, 'sp', 'tp'), may hold values from -0.125 to 0.125
- norm_gain: bfloat16 [2048], replicated, may hold values from 0.099609375 to 1.8984375
- w_x: bfloat16 [2048, 2048], P('dp', 'tp'), may hold values from -0.125 to 0.125
- w_b: bfloat16 [2048, 512], P('dp', 'tp'), may hold values from -0.125 to 0.125
- w_c: bfloat16 [2048, 512], P('dp', 'tp'), may hold values from -0.125 to 0.125
- w_z: bfloat16 [2048, 2048], P('dp', 'tp'), may hold values from -0.125 to 0.125
- w_dt: bfloat16 [2, 2048, 32], P(None, 'dp', 'tp'), may hold values from -0.125 to 0.125
- conv_x: bfloat16 [3, 2048], P(None, 'tp'), may hold values from -3.5 to 3.5
- conv_b: bfloat16 [3, 512], P(None, 'tp'), may hold values from -3.5 to 3.5
- conv_c: bfloat16 [3, 512], P(None, 'tp'), may hold values from -3.5 to 3.5
- decay_rate: float32 [2, 32], P(None, 'tp'), may hold values from 0 to 1, as said below
- out_gain: bfloat16 [2048], P('tp'), may hold values from 0.099609375 to 1.8984375
- w_out: bfloat16 [2048, 2048], P(('tp', 'dp')), may hold values from -0.125 to 0.125
Outputs:
- update: bfloat16 [2, 8192, 2048], P('dp', ('sp', 'tp'))
The draws below stay inside these ranges and needn't reach their ends.
Inputs may be any that keep to these rules, and one draw needn't show every extreme that they name: `decay_rate`: positive rates.
All inputs are finite; a program needn't handle non-finite values.
Results may differ from the reference program's by a relative error of at most 0.014.
Values may be sent and summed in bfloat16 or wider, within the bound.
A program may use at most 128 MiB of HBM per device.

```python
import jax
import jax.numpy as jnp
from jax import lax

D = 2048
HEADS = 32
HEAD_DIM = 64
GROUPS = 4
STATE = 128
CONV = 3
BLOCK = 128
TOK_DEV = 128
CTX = 512
INNER = 2048
SEQ = 8192
BATCH = 2
N_TP = 4


def draw_latent(key, part):
    noise_key, dir_key, span_key, block_key = jax.random.split(key, 4)
    shape = (BATCH, SEQ, D)
    noise = jax.random.truncated_normal(noise_key, -4.0, 4.0, shape, jnp.float32)
    direction = jax.random.truncated_normal(dir_key, -3.0, 3.0, (D,), jnp.float32)
    coarse = jnp.repeat(jax.random.uniform(span_key, (BATCH, SEQ // TOK_DEV, 1), jnp.float32, -1.5, 1.5), TOK_DEV, axis=1)
    finer = jnp.repeat(jax.random.uniform(block_key, (BATCH, SEQ // BLOCK, 1), jnp.float32, -0.5, 0.5), BLOCK, axis=1)
    return (noise + (coarse + finer) * direction).astype(jnp.bfloat16)


def draw_decay_rate(key, part):
    slow_key, fast_key, pick_key = jax.random.split(key, 3)
    chain = SEQ + CTX
    slow_rate = jax.random.uniform(slow_key, (2, HEADS), jnp.float32, 0.6, 2.0) / chain
    fast_rate = jax.random.uniform(fast_key, (2, HEADS), jnp.float32, 0.015, 0.04)
    picked = jax.random.uniform(pick_key, (2, HEADS), jnp.float32) < 0.25
    return jnp.where(picked, fast_rate, slow_rate)


def levels(rng, shape, cuts, smallest, top_value):
    def one(axis_at, blocks):
        steps = jax.random.uniform(jax.random.fold_in(jax.random.fold_in(rng, 6), axis_at), (blocks,), jnp.float32, smallest / len(cuts), top_value / len(cuts))
        return jnp.repeat(jnp.exp(steps), shape[axis_at] // blocks).reshape((-1,) + (1,) * (len(shape) - axis_at - 1))

    loudness = one(*cuts[0])
    for cut in cuts[1:]:
        loudness = loudness * one(*cut)
    return loudness


def gaussian(rng, shape, scale, limit, cuts=(), held_as=jnp.bfloat16):
    values = jax.random.normal(rng, shape, jnp.float32) * scale
    if len(cuts) > 0:
        values = levels(rng, shape, cuts, -0.22, 0.18) * values
    return jnp.clip(values, min=-limit, max=limit).astype(held_as)


def setup_inputs(seed: int = 0) -> dict:
    key_of = jax.random.split(jax.random.key(seed), 18)
    latent = draw_latent(jax.random.fold_in(key_of[17], 71), 0)
    condition = gaussian(key_of[1], (BATCH, D), 1.0, 6.0, ((0, 2),))
    context = gaussian(key_of[2], (BATCH, CTX, D), 1.0, 6.0, ((0, 2), (1, 64)))
    context_source = gaussian(key_of[3], (D,), 1.0, 6.0)
    mod_weight = gaussian(key_of[4], (3, D, D), D ** -0.5, 0.125, ((1, 64), (2, 4)))
    norm_gain = jnp.clip(1.0 + 0.18 * jax.random.normal(key_of[5], (D,), jnp.float32), 0.099609375, 1.8984375).astype(jnp.bfloat16)
    w_x = gaussian(key_of[6], (D, INNER), D ** -0.5, 0.125, ((0, 2), (1, 4)))
    w_b = gaussian(key_of[7], (D, GROUPS * STATE), D ** -0.5, 0.125, ((0, 2), (1, 4)))
    w_c = gaussian(key_of[8], (D, GROUPS * STATE), D ** -0.5, 0.125, ((0, 2), (1, 4)))
    w_z = gaussian(key_of[9], (D, INNER), D ** -0.5, 0.125, ((0, 2), (1, 4)))
    w_dt = gaussian(key_of[10], (2, D, HEADS), D ** -0.5, 0.125, ((1, 2), (2, 4)))
    conv_x = gaussian(key_of[11], (CONV, INNER), CONV ** -0.5, 3.5, ((1, 4),))
    conv_b = gaussian(key_of[12], (CONV, GROUPS * STATE), CONV ** -0.5, 3.5, ((1, 4),))
    conv_c = gaussian(key_of[13], (CONV, GROUPS * STATE), CONV ** -0.5, 3.5, ((1, 4),))
    decay_rate = draw_decay_rate(jax.random.fold_in(key_of[17], 71), 0)
    out_gain = jnp.clip(1.0 + 0.18 * jax.random.normal(key_of[15], (INNER,), jnp.float32), 0.099609375, 1.8984375).astype(jnp.bfloat16)
    w_out = gaussian(key_of[16], (INNER, D), INNER ** -0.5, 0.125, ((0, 8),))
    return dict(latent=latent, condition=condition, context=context, context_source=context_source, mod_weight=mod_weight, norm_gain=norm_gain, w_x=w_x, w_b=w_b, w_c=w_c, w_z=w_z, w_dt=w_dt, conv_x=conv_x, conv_b=conv_b, conv_c=conv_c, decay_rate=decay_rate, out_gain=out_gain, w_out=w_out)


EPSILON = 1e-06

def rounded(values):
    return lax.optimization_barrier(values.astype(jnp.bfloat16)).astype(jnp.float32)

def modulated(source, gain_vec, shift_vec, scale_vec):
    values = source.astype(jnp.float32)
    normed = values * lax.rsqrt(lax.optimization_barrier(jnp.mean(values * values, axis=-1, keepdims=True)) + EPSILON)
    return (normed * gain_vec.astype(jnp.float32) * (1.0 + scale_vec) + shift_vec).astype(jnp.bfloat16)

def project(source, weight):
    return jnp.dot(source, weight, preferred_element_type=jnp.float32).astype(jnp.bfloat16)

def centred_conv(source, weight):
    total_rows = source.shape[0]
    reach_rows = weight.shape[0] // 2
    padded = jnp.pad(source.astype(jnp.float32), ((reach_rows, reach_rows), (0, 0)))
    tap_weights = weight.astype(jnp.float32)
    summed = jnp.zeros(source.shape, jnp.float32)
    for offset in range(weight.shape[0]):
        summed = summed + padded[offset:offset + total_rows] * tap_weights[offset]
    return jax.nn.silu(summed).astype(jnp.bfloat16)

def final_state(x_vals, b_vals, step_size, rate_head):
    total_rows, head_count = step_size.shape
    per_group = head_count // GROUPS
    moved_x = rounded(x_vals.reshape(total_rows, head_count, HEAD_DIM).astype(jnp.float32) * step_size[:, :, None])
    running = jnp.cumsum(-rate_head * step_size, axis=0)
    weight = jnp.exp(running[-1:] - running)
    scaled = (moved_x * weight[:, :, None]).reshape(total_rows, GROUPS, per_group, HEAD_DIM)
    b_wide = b_vals.reshape(total_rows, GROUPS, STATE).astype(jnp.float32)
    return jnp.einsum('sgn,sghp->ghpn', b_wide, scaled, precision=lax.Precision.HIGHEST)

def ssd_direction(x_vals, b_vals, c_vals, step_size, rate_head, start_state):
    total_rows, head_count = step_size.shape
    per_group = head_count // GROUPS
    blocks = total_rows // BLOCK
    moved_x = rounded(x_vals.reshape(total_rows, head_count, HEAD_DIM).astype(jnp.float32) * step_size[:, :, None])
    decay_log = -rate_head * step_size
    lower_part = jnp.arange(BLOCK)[:, None] >= jnp.arange(BLOCK)[None, :]

    def advance(carried_in, inputs):
        x_block, b_block, c_block, d_block = inputs
        running = jnp.cumsum(d_block, axis=0)
        across = running.T
        spread = across[:, :, None] - across[:, None, :]
        decay_mask = jnp.where(lower_part, jnp.exp(jnp.minimum(spread, 0.0)), 0.0).reshape(GROUPS, per_group, BLOCK, BLOCK)
        b_wide = b_block.astype(jnp.float32)
        c_wide = c_block.astype(jnp.float32)
        scores = jnp.einsum('lgn,sgn->gls', c_wide, b_wide)
        weights = rounded(scores[:, None] * decay_mask)
        x_group = x_block.reshape(BLOCK, GROUPS, per_group, HEAD_DIM)
        inside = jnp.einsum('ghls,sghp->lghp', weights, x_group)
        carried = jnp.einsum('lgn,ghpn->lghp', c_wide, rounded(carried_in))
        growth = jnp.exp(running).reshape(BLOCK, GROUPS, per_group, 1)
        to_end = jnp.exp(running[-1:] - running).reshape(BLOCK, GROUPS, per_group, 1)
        fresh_state = jnp.einsum('sgn,sghp->ghpn', b_wide, rounded(x_group * to_end))
        ending = carried_in * jnp.exp(running[-1]).reshape(GROUPS, per_group, 1, 1) + fresh_state
        return (ending, inside + growth * carried)
    _, outputs = lax.scan(advance, start_state, (moved_x.reshape(blocks, BLOCK, head_count, HEAD_DIM), b_vals.reshape(blocks, BLOCK, GROUPS, STATE), c_vals.reshape(blocks, BLOCK, GROUPS, STATE), decay_log.reshape(blocks, BLOCK, head_count)))
    return outputs.reshape(total_rows, head_count * HEAD_DIM)

def reference(latent, condition, context, context_source, mod_weight, norm_gain, w_x, w_b, w_c, w_z, w_dt, conv_x, conv_b, conv_c, decay_rate, out_gain, w_out):
    activation = rounded(jax.nn.silu(condition.astype(jnp.float32)))
    source_act = rounded(jax.nn.silu(context_source.astype(jnp.float32)))
    weight_wide = mod_weight.astype(jnp.float32)
    mod_latent = jnp.einsum('bd,kdc->kbc', activation, weight_wide)
    mod_context = jnp.einsum('d,kdc->kc', source_act, weight_wide)
    part_width = INNER // N_TP
    outputs = []
    for sample in range(latent.shape[0]):
        ctx_rows = modulated(context[sample], norm_gain, mod_context[0], mod_context[1])
        ctx_x = centred_conv(project(ctx_rows, w_x), conv_x)
        ctx_b = centred_conv(project(ctx_rows, w_b), conv_b)
        ctx_fwd = jax.nn.softplus(project(ctx_rows, w_dt[0]).astype(jnp.float32))
        ctx_bwd = jax.nn.softplus(project(ctx_rows, w_dt[1]).astype(jnp.float32))
        state_fwd = final_state(ctx_x, ctx_b, ctx_fwd, decay_rate[0])
        state_bwd = final_state(jnp.flip(ctx_x, 0), jnp.flip(ctx_b, 0), jnp.flip(ctx_bwd, 0), decay_rate[1])
        latent_rows = modulated(latent[sample], norm_gain, mod_latent[0, sample], mod_latent[1, sample])
        x_vals = centred_conv(project(latent_rows, w_x), conv_x)
        b_vals = centred_conv(project(latent_rows, w_b), conv_b)
        c_vals = centred_conv(project(latent_rows, w_c), conv_c)
        step_fwd = jax.nn.softplus(project(latent_rows, w_dt[0]).astype(jnp.float32))
        step_bwd = jax.nn.softplus(project(latent_rows, w_dt[1]).astype(jnp.float32))
        gate_in = project(latent_rows, w_z)
        total_rows = latent_rows.shape[0]
        out_fwd = ssd_direction(x_vals, b_vals, c_vals, step_fwd, decay_rate[0], state_fwd)
        out_bwd = jnp.flip(ssd_direction(jnp.flip(x_vals, 0), jnp.flip(b_vals, 0), jnp.flip(c_vals, 0), jnp.flip(step_bwd, 0), decay_rate[1], state_bwd), 0)
        gated = (out_fwd + out_bwd) * jax.nn.silu(gate_in.astype(jnp.float32))
        grouped = gated.reshape(total_rows, GROUPS, -1)
        normed = grouped * lax.rsqrt(lax.optimization_barrier(jnp.mean(grouped * grouped, axis=-1, keepdims=True)) + EPSILON) * out_gain.reshape(GROUPS, -1).astype(jnp.float32)
        normed_out = normed.reshape(total_rows, -1).astype(jnp.bfloat16)
        mixed = jnp.zeros((total_rows, w_out.shape[1]), jnp.float32)
        for part_idx in range(N_TP):
            lower_col = part_idx * part_width
            term = jnp.dot(normed_out[:, lower_col:lower_col + part_width], w_out[lower_col:lower_col + part_width], preferred_element_type=jnp.float32)
            mixed = mixed + rounded(term)
        outputs.append((mod_latent[2, sample] * mixed).astype(jnp.bfloat16))
    return jnp.stack(outputs)
```

```python
import functools

import jax
import jax.numpy as jnp
from jax import lax
from jax.experimental import pallas as pl
from jax.experimental.pallas import tpu as pltpu
from jax.sharding import PartitionSpec as P

STATE = 128
LANES = 128
PAD = 16
SIDE = 8
TILE = 16
EPSILON = 1e-06
MESH = pl.DeviceIdType.MESH
F32 = jnp.float32
BF16 = jnp.bfloat16


def silu(v):
    return v / (1.0 + jnp.exp(-v))


def softplus(v):
    return jnp.maximum(v, 0.0) + jnp.log1p(jnp.exp(-jnp.abs(v)))


def row_of(ref):
    return ref[...].astype(F32).reshape(1, ref.shape[0])


def dot(a, b, dims=((1,), (0,)), precision=None):
    return lax.dot_general(a, b, (dims, ((), ())), precision=precision, preferred_element_type=F32)


def far_first():
    def reach(k):
        return min(k, SIDE - k)

    steps = [(a, b) for a in range(SIDE) for b in range(SIDE) if a or b]
    return sorted(steps, key=lambda ab: -(reach(ab[0]) + reach(ab[1])))


def kernel(
    n_sp,
    n_tp,
    n_dp,
    heads,
    condition_in,
    source_in,
    gain_in,
    conv_x_in,
    conv_b_in,
    conv_c_in,
    rate_in,
    out_gain_in,
    latent,
    context,
    mod_weight,
    w_x,
    w_b,
    w_c,
    w_dt,
    w_z,
    w_out,
    out,
    condition,
    source,
    gain,
    conv_x,
    conv_b,
    conv_c,
    rate,
    out_gain,
    lat_all,
    ctx_buf,
    mod_buf,
    wx,
    wb,
    wc,
    wd,
    wz,
    wo,
    acts,
    edges,
    part,
    part_z,
    part_up,
    part_y,
    mods,
    halo,
    pre,
    hid,
    snd_c,
    rcv_c,
    snd_l,
    rcv_l,
    snd_t,
    rcv_t,
    snd_b,
    rcv_b,
    snd_o,
    rcv_o,
    local_sem,
    dp_send,
    dp_recv,
    lat_send,
    lat_recv,
    line_send,
    line_recv,
    mod_send,
    mod_recv,
    edge_send,
    edge_recv,
    flat_send,
    flat_recv,
    o_send,
    o_recv,
):
    s = lax.axis_index("sp")
    t = lax.axis_index("tp")
    d = lax.axis_index("dp")
    z = s // SIDE
    y = lax.rem(s, SIDE)
    own_rows, width = latent.shape
    ctx_rows = context.shape[0]
    depth = mod_weight.shape[1]
    rows = n_tp * own_rows
    inner = w_x.shape[1]
    both = 2 * inner
    head_dim = inner // heads
    nh2 = 2 * heads
    up, down = lax.rem(s + 1, n_sp), lax.rem(s + n_sp - 1, n_sp)

    def remote(src, dst, send, recv, **to):
        return pltpu.make_async_remote_copy(
            src_ref=src, dst_ref=dst, send_sem=send, recv_sem=recv, device_id=to, device_id_type=MESH
        )

    barrier = pltpu.get_barrier_semaphore()

    def greet(**to):
        pl.semaphore_signal(barrier, inc=1, device_id=to, device_id_type=MESH)

    def on_z(k):
        return lax.rem(z + k, SIDE) * SIDE + y

    def on_y(k):
        return z * SIDE + lax.rem(y + k, SIDE)

    for k in range(1, SIDE):
        greet(sp=on_z(k))
        greet(sp=on_y(k))
    for k in range(1, n_tp):
        greet(tp=lax.rem(t + k, n_tp))
    for k in range(1, n_dp):
        greet(dp=lax.rem(d + k, n_dp))
    greet(sp=up)
    greet(sp=down)
    greet(sp=down, tp=n_tp - 1)
    greet(sp=up, tp=0)

    local = []

    def fetch(src, dst):
        copy = pltpu.make_async_copy(src, dst, local_sem.at[len(local)])
        copy.start()
        local.append(copy)
        return copy

    early = [fetch(condition_in, condition), fetch(source_in, source), fetch(mod_weight, mod_buf)]
    lat_copy = fetch(latent, lat_all.at[t])
    ctx_copy = fetch(context, ctx_buf)
    small = [
        fetch(a, b)
        for a, b in (
            (gain_in, gain),
            (conv_x_in, conv_x),
            (conv_b_in, conv_b),
            (conv_c_in, conv_c),
            (rate_in, rate),
            (out_gain_in, out_gain),
        )
    ]
    pairs = ((w_x, wx), (w_b, wb), (w_dt, wd), (w_c, wc), (w_z, wz), (w_out, wo))
    places = []
    weight_copies = []
    for src, dst in pairs:
        count = src.shape[0]
        places.append(dst.at[d] if src is w_dt else dst.at[pl.ds(d * count, count)])
        weight_copies.append(fetch(src, places[-1]))

    for copy in early:
        copy.wait()
    acts[0:1] = condition[...].astype(F32)
    acts[1:2] = row_of(source)
    per = LANES // depth
    block = acts[0:2, pl.ds(pl.multiple_of((s // per) * LANES, LANES), LANES)]
    active = jnp.concatenate([silu(block), jnp.zeros((PAD - 2, LANES), F32)], axis=0)
    own_acts = active[:, 0:depth]
    for j in range(1, per):
        own_acts = jnp.where(lax.rem(s, per) == j, active[:, j * depth : (j + 1) * depth], own_acts)
    own_acts = own_acts.astype(BF16)
    pieces = [dot(own_acts, mod_buf[k])[0:2] for k in range(mod_buf.shape[0])]
    cols = pieces[0].shape[1]
    partial = jnp.concatenate(pieces + [jnp.zeros((2, cols), F32)], axis=0)
    part[...] = partial

    lat_copy.wait()
    edges[0] = lat_all[t, 0:1].astype(F32)
    edges[1] = lat_all[t, own_rows - 1 : own_rows].astype(F32)
    ctx_copy.wait()
    edges[2] = ctx_buf[0:1].astype(F32)
    edges[3] = ctx_buf[ctx_rows - 1 : ctx_rows].astype(F32)

    expected = 2 * (SIDE - 1) + n_tp - 1 + n_dp - 1 + 2
    expected = expected + jnp.where(t == n_tp - 1, n_tp, 0) + jnp.where(t == 0, n_tp, 0)
    pl.semaphore_wait(barrier, expected)

    def line(src, dst, place, phase):
        for k in range(1, SIDE):
            remote(src, dst.at[k - 1], line_send.at[phase], line_recv.at[phase], sp=place(k)).start()

    def line_wait(dst, phase):
        pltpu.make_async_copy(dst, dst, line_recv.at[phase]).wait()

    line(part, part_z, on_z, 0)
    lat_moves = []
    for k in range(1, n_tp):
        lat_moves.append(
            remote(latent, lat_all.at[t], lat_send.at[k], lat_recv.at[k], tp=lax.rem(t + k, n_tp))
        )
        lat_moves[-1].start()
    ctx_up = remote(edges.at[3], halo.at[2], edge_send.at[0], edge_recv.at[2], sp=up)
    ctx_down = remote(edges.at[2], halo.at[3], edge_send.at[1], edge_recv.at[3], sp=down)
    ctx_up.start()
    ctx_down.start()
    lat_up = [
        remote(edges.at[1], halo.at[0], edge_send.at[2 + u], edge_recv.at[0], sp=up, tp=u)
        for u in range(n_tp)
    ]
    lat_down = [
        remote(edges.at[0], halo.at[1], edge_send.at[2 + n_tp + u], edge_recv.at[1], sp=down, tp=u)
        for u in range(n_tp)
    ]

    @pl.when(t == n_tp - 1)
    def _():
        for copy in lat_up:
            copy.start()

    @pl.when(t == 0)
    def _():
        for copy in lat_down:
            copy.start()

    weight_moves = []
    for i, (src, dst) in enumerate(pairs):
        for k in range(1, n_dp):
            at = i * n_dp + k
            weight_moves.append(
                remote(src, places[i], dp_send.at[at], dp_recv.at[at], dp=lax.rem(d + k, n_dp))
            )
            weight_moves[-1].start()

    def normed(v):
        return v * lax.rsqrt(jnp.mean(v * v, axis=1, keepdims=True) + EPSILON)

    pre[rows + PAD : rows + PAD + ctx_rows] = normed(ctx_buf[...].astype(F32))

    line_wait(part_z, 0)
    summed = part[...]
    for k in range(1, SIDE):
        summed = summed + part_z[k - 1]
    part_up[...] = summed
    line(part_up, part_y, on_y, 1)

    for copy in lat_moves:
        copy.wait()
    for u in range(n_tp):
        pre[u * own_rows : (u + 1) * own_rows] = normed(lat_all[u].astype(F32))
    ctx_up.wait_recv()
    ctx_down.wait_recv()
    lat_up[0].wait_recv()
    lat_down[0].wait_recv()
    pre[rows : rows + PAD] = normed(
        jnp.concatenate([halo[0], halo[1], halo[2], halo[3], jnp.zeros((PAD - 4, width), F32)], axis=0)
    )

    line_wait(part_y, 1)
    summed = part_up[...]
    for k in range(1, SIDE):
        summed = summed + part_y[k - 1]
    mods[t] = summed
    moves = []
    for k in range(1, n_tp):
        moves.append(
            remote(mods.at[t], mods.at[t], mod_send.at[k], mod_recv.at[k], tp=lax.rem(t + k, n_tp))
        )
        moves[-1].start()
    for copy in small:
        copy.wait()
    for copy in moves:
        copy.wait()

    def vector(row):
        return jnp.concatenate([mods[c][row : row + 1] for c in range(n_tp)], axis=1)

    gain_row = row_of(gain)
    lat_shift, ctx_shift = vector(0), vector(1)
    lat_gain = gain_row * (1.0 + vector(2))
    ctx_gain = gain_row * (1.0 + vector(3))
    for u in range(n_tp):
        cut = slice(u * own_rows, (u + 1) * own_rows)
        hid[cut] = (pre[cut] * lat_gain + lat_shift).astype(BF16)
    at_row = lax.broadcasted_iota(jnp.int32, (PAD, width), 0)
    edge = pre[rows : rows + PAD]
    hid[rows : rows + PAD] = jnp.where(
        at_row < 2, edge * lat_gain + lat_shift, edge * ctx_gain + ctx_shift
    ).astype(BF16)
    hid[rows + PAD : rows + PAD + ctx_rows] = (
        pre[rows + PAD : rows + PAD + ctx_rows] * ctx_gain + ctx_shift
    ).astype(BF16)
    for copy in weight_moves:
        copy.wait()
    for copy in weight_copies:
        copy.wait()

    has_before = s > 0
    has_after = s < n_sp - 1

    def shaped(values, before, after, taps):
        count = values.shape[0]
        at = lax.broadcasted_iota(jnp.int32, values.shape, 0)
        before = jnp.where(has_before, before, 0.0)
        after = jnp.where(has_after, after, 0.0)
        earlier = jnp.where(at == 0, before, pltpu.roll(values, 1, 0))
        later = jnp.where(at == count - 1, after, pltpu.roll(values, count - 1, 0))
        w = taps[...].astype(F32)
        return silu(earlier * w[0:1] + values * w[1:2] + later * w[2:3]).astype(BF16)

    def project(weight, count):
        return dot(hid[0:count], weight[...]).astype(BF16).astype(F32)

    total = rows + PAD + ctx_rows
    spread_at = lax.broadcasted_iota(jnp.int32, (LANES, both), 0)
    spread_to = lax.broadcasted_iota(jnp.int32, (LANES, both), 1) // head_dim
    spreader = jnp.where((spread_to == spread_at) | (spread_to + nh2 == spread_at), 1.0, 0.0).astype(BF16)

    def expand(v):
        lane = lax.broadcasted_iota(jnp.int32, v.shape, 1)
        high = v.astype(BF16).astype(F32)
        low = pltpu.roll(v - high, nh2, 1)
        packed = jnp.where(lane < nh2, high, jnp.where(lane < 2 * nh2, low, 0.0))
        return dot(packed.astype(BF16), spreader)

    def running(steps):
        count = steps.shape[0]
        logs = -rates * steps
        a = lax.broadcasted_iota(jnp.int32, (count, count), 0)
        b = lax.broadcasted_iota(jnp.int32, (count, count), 1)
        lower = jnp.where(a >= b, 1.0, 0.0)
        upper = jnp.where(a <= b, 1.0, 0.0)
        lane = lax.broadcasted_iota(jnp.int32, logs.shape, 1)
        sums = jnp.where(
            lane < heads,
            dot(lower, logs, precision=lax.Precision.HIGHEST),
            dot(upper, logs, precision=lax.Precision.HIGHEST),
        )
        row_lane = lax.broadcasted_iota(jnp.int32, (1, LANES), 1)
        ends = jnp.where(row_lane < heads, sums[count - 1 : count], sums[0:1])
        return sums, ends

    def moved(values, steps):
        wide = jnp.concatenate([values, values], axis=1)
        return (wide * expand(steps)).astype(BF16)

    def spread_out(src, dst, phase):
        for a, b in far_first():
            to = lax.rem(z + a, SIDE) * SIDE + lax.rem(y + b, SIDE)
            remote(src.at[to], dst.at[s], flat_send.at[phase], flat_recv.at[phase], sp=to).start()
        dst[s] = src[s]

    def all_in(dst, phase):
        most = dst.at[pl.ds(0, n_sp - 1)]
        pltpu.make_async_copy(most, most, flat_recv.at[phase]).wait()

    def tiles(dst, state):
        for a in range(SIDE):
            for b in range(SIDE):
                dst[a * SIDE + b] = state[
                    b * TILE : (b + 1) * TILE, a * LANES : (a + 1) * LANES
                ].astype(BF16)

    features = None
    half = wd.shape[3]
    for r in range(n_dp):
        taps = jnp.concatenate(
            [wd[r, 0].astype(F32), wd[r, 1].astype(F32), jnp.zeros((LANES - nh2, half), F32)], axis=0
        ).astype(BF16)
        one = dot(hid[0:total, r * half : (r + 1) * half], taps, ((1,), (1,)))
        features = one if features is None else features + one
    step_all = softplus(features.astype(BF16).astype(F32))
    rates = jnp.concatenate([rate[0:1], rate[1:2], jnp.zeros((1, LANES - nh2), F32)], axis=1)
    c_steps = step_all[rows + PAD :]
    c_sums, c_ends = running(c_steps)
    l_steps = step_all[0:rows]
    l_sums, l_ends = running(l_steps)
    ends = expand(jnp.exp(jnp.concatenate([c_ends, l_ends, jnp.zeros((6, LANES), F32)], axis=0)))
    for a in range(SIDE):
        lanes = ends[0:2, a * LANES : (a + 1) * LANES]
        for b in range(SIDE):
            snd_t[a * SIDE + b] = lanes
    spread_out(snd_t, rcv_t, 0)

    px = project(wx, total)
    cx_in = shaped(
        px[rows + PAD :], px[rows + 2 : rows + 3], px[rows + 3 : rows + 4], conv_x
    ).astype(F32)
    pb = project(wb, total)
    cb_in = shaped(pb[rows + PAD :], pb[rows + 2 : rows + 3], pb[rows + 3 : rows + 4], conv_b)
    c_moved = moved(cx_in, c_steps)
    c_scaled = (c_moved.astype(F32) * expand(jnp.exp(c_ends - c_sums))).astype(BF16)
    tiles(snd_c, dot(cb_in, c_scaled, ((0,), (0,))))
    spread_out(snd_c, rcv_c, 1)

    x_in = shaped(px[0:rows], px[rows : rows + 1], px[rows + 1 : rows + 2], conv_x).astype(F32)
    b_in = shaped(pb[0:rows], pb[rows : rows + 1], pb[rows + 1 : rows + 2], conv_b)
    l_moved = moved(x_in, l_steps)
    l_scaled = (l_moved.astype(F32) * expand(jnp.exp(l_ends - l_sums))).astype(BF16)
    tiles(snd_l, dot(b_in, l_scaled, ((0,), (0,))))
    spread_out(snd_l, rcv_l, 2)

    pc = project(wc, rows + PAD)
    c_in = shaped(pc[0:rows], pc[rows : rows + 1], pc[rows + 1 : rows + 2], conv_c)
    scores = dot(c_in, b_in, ((1,), (1,)))
    at_t = lax.broadcasted_iota(jnp.int32, (rows, rows), 0)
    at_s = lax.broadcasted_iota(jnp.int32, (rows, rows), 1)
    sums_t = jnp.transpose(l_sums)

    def weights(lane, keep):
        gap = l_sums[:, lane : lane + 1] - sums_t[lane : lane + 1]
        return jnp.where(keep, scores * jnp.exp(jnp.minimum(gap, 0.0)), 0.0).astype(BF16)

    pair = LANES // head_dim
    inside = []
    lane_head = lax.broadcasted_iota(jnp.int32, (rows, LANES), 1) // head_dim
    for p in range(heads // pair):
        cut = slice(p * LANES, (p + 1) * LANES)
        cut_b = slice(inner + p * LANES, inner + (p + 1) * LANES)
        sources = jnp.concatenate([l_moved[:, cut], l_moved[:, cut_b]], axis=0)
        value = None
        for i in range(pair):
            h = p * pair + i
            w = jnp.concatenate([weights(h, at_t >= at_s), weights(heads + h, at_t <= at_s)], axis=1)
            one = dot(w, sources)
            value = one if value is None else jnp.where(lane_head == i, one, value)
        inside.append(value)
    inside = jnp.concatenate(inside, axis=1)
    growth = expand(jnp.exp(l_sums))
    gate = silu(project(wz, rows))

    forward = z < SIDE // 2

    def place(j):
        return jnp.where(forward, j, n_sp - 1 - j)

    all_in(rcv_t, 0)
    all_in(rcv_c, 1)
    state = jnp.zeros((TILE, LANES), F32)

    def context_step(j, state):
        i = place(j)
        return state * rcv_t[i, 0:1] + rcv_c[i].astype(F32)

    state = lax.fori_loop(0, n_sp, context_step, state, unroll=8)
    all_in(rcv_l, 2)

    def latent_step(j, state):
        i = place(j)
        snd_b[i] = state.astype(BF16)
        return state * rcv_t[i, 1:2] + rcv_l[i].astype(F32)

    lax.fori_loop(0, n_sp, latent_step, state, unroll=8)
    spread_out(snd_b, rcv_b, 3)
    all_in(rcv_b, 3)
    entering = jnp.concatenate(
        [rcv_b[a * SIDE : (a + 1) * SIDE].reshape(STATE, LANES) for a in range(SIDE)], axis=1
    )
    carried = dot(c_in, entering) * growth
    gated = (inside + carried[:, 0:inner] + carried[:, inner:both]) * gate
    ny = (
        gated
        * lax.rsqrt(jnp.mean(gated * gated, axis=1, keepdims=True) + EPSILON)
        * row_of(out_gain)
    ).astype(BF16)

    chunks = n_tp
    chunk = width // chunks
    o_moves = []
    for c in range(chunks):
        cut = slice(c * chunk, (c + 1) * chunk)
        result = dot(ny, wo[:, cut]).astype(BF16)
        for u in range(n_tp):
            snd_o[c, u] = result[u * own_rows : (u + 1) * own_rows]
        for k in range(1, n_tp):
            to = lax.rem(t + k, n_tp)
            at = c * n_tp + k
            o_moves.append(remote(snd_o.at[c, to], rcv_o.at[c, k], o_send.at[at], o_recv.at[at], tp=to))
            o_moves[-1].start()

    for phase, sent in ((0, part_z), (1, part_y)):
        pltpu.make_async_copy(sent, sent, line_send.at[phase]).wait()
    for phase, sent in ((0, rcv_t), (1, rcv_c), (2, rcv_l), (3, rcv_b)):
        most = sent.at[pl.ds(0, n_sp - 1)]
        pltpu.make_async_copy(most, most, flat_send.at[phase]).wait()
    ctx_up.wait_send()
    ctx_down.wait_send()

    @pl.when(t == n_tp - 1)
    def _():
        for copy in lat_up:
            copy.wait_send()

    @pl.when(t == 0)
    def _():
        for copy in lat_down:
            copy.wait_send()

    for c in range(chunks):
        mixed = snd_o[c, t].astype(F32)
        for k in range(1, n_tp):
            o_moves[c * (n_tp - 1) + k - 1].wait()
            mixed = mixed + rcv_o[c, k].astype(F32)
        out[:, c * chunk : (c + 1) * chunk] = (mods[c][4:5] * mixed).astype(BF16)


def shards(
    latent,
    condition,
    context,
    context_source,
    mod_weight,
    norm_gain,
    w_x,
    w_b,
    w_c,
    w_z,
    w_dt,
    conv_x,
    conv_b,
    conv_c,
    decay_rate,
    out_gain,
    w_out,
):
    n_sp, n_tp, n_dp = lax.axis_size("sp"), lax.axis_size("tp"), lax.axis_size("dp")
    assert n_sp == SIDE * SIDE
    own_rows, width = latent.shape[1:]
    ctx_rows = context.shape[1]
    cols = mod_weight.shape[2]
    inner = w_x.shape[1]
    heads = decay_rate.shape[1]
    assert STATE == SIDE * TILE and 2 * inner == SIDE * LANES
    rows = n_tp * own_rows
    total = rows + PAD + ctx_rows
    chunk = width // n_tp
    vmem = pl.BlockSpec(memory_space=pltpu.VMEM)
    anywhere = pl.BlockSpec(memory_space=pl.ANY)
    dma = pltpu.SemaphoreType.DMA
    args = (
        condition,
        context_source,
        norm_gain,
        conv_x,
        conv_b,
        conv_c,
        decay_rate,
        out_gain,
        latent[0],
        context[0],
        mod_weight,
        w_x,
        w_b,
        w_c,
        jnp.swapaxes(w_dt, 1, 2),
        w_z,
        w_out,
    )
    tiles = pltpu.VMEM((n_sp, TILE, LANES), BF16)
    scratch = [pltpu.VMEM(a.shape, a.dtype) for a in args[:8]] + [
        pltpu.VMEM((n_tp, own_rows, width), BF16),
        pltpu.VMEM((ctx_rows, width), BF16),
        pltpu.VMEM(mod_weight.shape, BF16),
        pltpu.VMEM((w_x.shape[0] * n_dp, inner), BF16),
        pltpu.VMEM((w_b.shape[0] * n_dp, w_b.shape[1]), BF16),
        pltpu.VMEM((w_c.shape[0] * n_dp, w_c.shape[1]), BF16),
        pltpu.VMEM((n_dp, 2, heads, w_dt.shape[1]), BF16),
        pltpu.VMEM((w_z.shape[0] * n_dp, inner), BF16),
        pltpu.VMEM((w_out.shape[0] * n_dp, width), BF16),
        pltpu.VMEM((8, width), F32),
        pltpu.VMEM((4, 1, width), F32),
        pltpu.VMEM((8, cols), F32),
        pltpu.VMEM((SIDE - 1, 8, cols), F32),
        pltpu.VMEM((8, cols), F32),
        pltpu.VMEM((SIDE - 1, 8, cols), F32),
        pltpu.VMEM((n_tp, 8, cols), F32),
        pltpu.VMEM((4, 1, width), F32),
        pltpu.VMEM((total, width), F32),
        pltpu.VMEM((total, width), BF16),
        tiles,
        tiles,
        tiles,
        tiles,
        pltpu.VMEM((n_sp, 2, LANES), F32),
        pltpu.VMEM((n_sp, 2, LANES), F32),
        tiles,
        tiles,
        pltpu.VMEM((n_tp, n_tp, own_rows, chunk), BF16),
        pltpu.VMEM((n_tp, n_tp, own_rows, chunk), BF16),
        dma((17,)),
        dma((6 * n_dp,)),
        dma((6 * n_dp,)),
        dma((n_tp,)),
        dma((n_tp,)),
        dma((2,)),
        dma((2,)),
        dma((n_tp,)),
        dma((n_tp,)),
        dma((2 + 2 * n_tp,)),
        dma((4,)),
        dma((4,)),
        dma((4,)),
        dma((n_tp * n_tp,)),
        dma((n_tp * n_tp,)),
    ]
    result = pl.pallas_call(
        functools.partial(kernel, n_sp, n_tp, n_dp, heads),
        out_shape=jax.ShapeDtypeStruct((own_rows, width), BF16),
        in_specs=[anywhere] * len(args),
        out_specs=vmem,
        scratch_shapes=scratch,
        compiler_params=pltpu.CompilerParams(
            collective_id=0, has_side_effects=True, vmem_limit_bytes=62_000_000
        ),
    )(*args)
    return result[None]


def solution(mesh):
    placed = (
        P("dp", ("sp", "tp"), None),
        P("dp", None),
        P("dp", "sp", None),
        P(),
        P(None, "sp", "tp"),
        P(),
        P("dp", "tp"),
        P("dp", "tp"),
        P("dp", "tp"),
        P("dp", "tp"),
        P(None, "dp", "tp"),
        P(None, "tp"),
        P(None, "tp"),
        P(None, "tp"),
        P(None, "tp"),
        P("tp"),
        P(("tp", "dp"), None),
    )
    return jax.shard_map(
        shards, mesh=mesh, in_specs=placed, out_specs=P("dp", ("sp", "tp"), None), check_vma=False
    )
```

```python
import functools

import jax
import jax.numpy as jnp
from jax import lax
from jax.experimental import pallas as pl
from jax.experimental.pallas import tpu as pltpu
from jax.sharding import PartitionSpec as P

STATE = 128
LANES = 128
PAD = 16
SIDE = 8
TILE = 16
EPSILON = 1e-06
MESH = pl.DeviceIdType.MESH
F32 = jnp.float32
BF16 = jnp.bfloat16


def silu(v):
    return v / (1.0 + jnp.exp(-v))


def softplus(v):
    return jnp.maximum(v, 0.0) + jnp.log1p(jnp.exp(-jnp.abs(v)))


def row_of(ref):
    return ref[...].astype(F32).reshape(1, ref.shape[0])


def dot(a, b, dims=((1,), (0,)), precision=None):
    return lax.dot_general(a, b, (dims, ((), ())), precision=precision, preferred_element_type=F32)


def far_first():
    def reach(k):
        return min(k, SIDE - k)

    steps = [(a, b) for a in range(SIDE) for b in range(SIDE) if a or b]
    return sorted(steps, key=lambda ab: -(reach(ab[0]) + reach(ab[1])))


def kernel(
    n_sp,
    n_tp,
    n_dp,
    heads,
    condition_in,
    source_in,
    gain_in,
    conv_x_in,
    conv_b_in,
    conv_c_in,
    rate_in,
    out_gain_in,
    latent,
    context,
    mod_weight,
    w_x,
    w_b,
    w_c,
    w_dt,
    w_z,
    w_out,
    out,
    condition,
    source,
    gain,
    conv_x,
    conv_b,
    conv_c,
    rate,
    out_gain,
    lat_all,
    ctx_buf,
    mod_buf,
    wx,
    wb,
    wc,
    wd,
    wz,
    wo,
    acts,
    edges,
    part,
    part_z,
    part_up,
    part_y,
    mods,
    halo,
    pre,
    hid,
    c_full,
    snd_c,
    rcv_c,
    snd_l,
    rcv_l,
    snd_t,
    rcv_t,
    snd_b,
    rcv_b,
    snd_o,
    rcv_o,
    local_sem,
    dp_send,
    dp_recv,
    lat_send,
    lat_recv,
    line_send,
    line_recv,
    mod_send,
    mod_recv,
    ctx_send,
    ctx_recv,
    edge_send,
    edge_recv,
    flat_send,
    flat_recv,
    o_send,
    o_recv,
):
    s = lax.axis_index("sp")
    t = lax.axis_index("tp")
    d = lax.axis_index("dp")
    z = s // SIDE
    y = lax.rem(s, SIDE)
    own_rows, width = latent.shape
    own_ctx = context.shape[0]
    ctx_rows = SIDE * own_ctx
    depth = mod_weight.shape[1]
    rows = n_tp * own_rows
    inner = w_x.shape[1]
    both = 2 * inner
    head_dim = inner // heads
    nh2 = 2 * heads
    up, down = lax.rem(s + 1, n_sp), lax.rem(s + n_sp - 1, n_sp)

    def remote(src, dst, send, recv, **to):
        return pltpu.make_async_remote_copy(
            src_ref=src, dst_ref=dst, send_sem=send, recv_sem=recv, device_id=to, device_id_type=MESH
        )

    barrier = pltpu.get_barrier_semaphore()

    def greet(**to):
        pl.semaphore_signal(barrier, inc=1, device_id=to, device_id_type=MESH)

    def on_z(k):
        return lax.rem(z + k, SIDE) * SIDE + y

    def on_y(k):
        return z * SIDE + lax.rem(y + k, SIDE)

    for k in range(1, SIDE):
        greet(sp=on_z(k))
        greet(sp=on_y(k))
    for k in range(1, n_tp):
        greet(tp=lax.rem(t + k, n_tp))
    for k in range(1, n_dp):
        greet(dp=lax.rem(d + k, n_dp))
    z_up, z_down = lax.rem(z + 1, SIDE) * SIDE, lax.rem(z + SIDE - 1, SIDE) * SIDE
    greet(sp=z_down + SIDE - 1)
    greet(sp=z_up)
    greet(sp=down, tp=n_tp - 1)
    greet(sp=up, tp=0)

    local = []

    def fetch(src, dst):
        copy = pltpu.make_async_copy(src, dst, local_sem.at[len(local)])
        copy.start()
        local.append(copy)
        return copy

    early = [fetch(condition_in, condition), fetch(source_in, source), fetch(mod_weight, mod_buf)]
    lat_copy = fetch(latent, lat_all.at[t])
    ctx_copy = fetch(context, ctx_buf.at[y])
    small = [
        fetch(a, b)
        for a, b in (
            (gain_in, gain),
            (conv_x_in, conv_x),
            (conv_b_in, conv_b),
            (conv_c_in, conv_c),
            (rate_in, rate),
            (out_gain_in, out_gain),
        )
    ]
    pairs = ((w_x, wx), (w_b, wb), (w_dt, wd), (w_c, wc), (w_z, wz), (w_out, wo))
    places = []
    weight_copies = []
    for src, dst in pairs:
        count = src.shape[0]
        places.append(dst.at[d] if src is w_dt else dst.at[pl.ds(d * count, count)])
        weight_copies.append(fetch(src, places[-1]))

    for copy in early:
        copy.wait()
    acts[0:1] = condition[...].astype(F32)
    acts[1:2] = row_of(source)
    per = LANES // depth
    block = acts[0:2, pl.ds(pl.multiple_of((s // per) * LANES, LANES), LANES)]
    active = jnp.concatenate([silu(block), jnp.zeros((PAD - 2, LANES), F32)], axis=0)
    own_acts = active[:, 0:depth]
    for j in range(1, per):
        own_acts = jnp.where(lax.rem(s, per) == j, active[:, j * depth : (j + 1) * depth], own_acts)
    own_acts = own_acts.astype(BF16)
    pieces = [dot(own_acts, mod_buf[k])[0:2] for k in range(mod_buf.shape[0])]
    cols = pieces[0].shape[1]
    partial = jnp.concatenate(pieces + [jnp.zeros((2, cols), F32)], axis=0)
    part[...] = partial.astype(BF16)

    lat_copy.wait()
    edges[0] = lat_all[t, 0:1].astype(F32)
    edges[1] = lat_all[t, own_rows - 1 : own_rows].astype(F32)
    ctx_copy.wait()
    edges[2] = ctx_buf[y, 0:1].astype(F32)
    edges[3] = ctx_buf[y, own_ctx - 1 : own_ctx].astype(F32)

    expected = 2 * (SIDE - 1) + n_tp - 1 + n_dp - 1
    expected = expected + jnp.where(y == SIDE - 1, SIDE, 0) + jnp.where(y == 0, SIDE, 0)
    expected = expected + jnp.where(t == n_tp - 1, n_tp, 0) + jnp.where(t == 0, n_tp, 0)
    pl.semaphore_wait(barrier, expected)

    def line(src, dst, place, phase):
        for k in range(1, SIDE):
            remote(src, dst.at[k - 1], line_send.at[phase], line_recv.at[phase], sp=place(k)).start()

    def line_wait(dst, phase):
        pltpu.make_async_copy(dst, dst, line_recv.at[phase]).wait()

    line(part, part_z, on_z, 0)
    lat_moves = []
    for k in range(1, n_tp):
        lat_moves.append(
            remote(latent, lat_all.at[t], lat_send.at[k], lat_recv.at[k], tp=lax.rem(t + k, n_tp))
        )
        lat_moves[-1].start()
    for k in range(1, SIDE):
        remote(context, ctx_buf.at[y], ctx_send.at[k], ctx_recv.at[k], sp=on_y(k)).start()
    ctx_up = [
        remote(edges.at[3], halo.at[2], edge_send.at[j], edge_recv.at[2], sp=z_up + j) for j in range(SIDE)
    ]
    ctx_down = [
        remote(edges.at[2], halo.at[3], edge_send.at[SIDE + j], edge_recv.at[3], sp=z_down + j)
        for j in range(SIDE)
    ]
    first = 2 * SIDE
    lat_up = [
        remote(edges.at[1], halo.at[0], edge_send.at[first + u], edge_recv.at[0], sp=up, tp=u)
        for u in range(n_tp)
    ]
    lat_down = [
        remote(edges.at[0], halo.at[1], edge_send.at[first + n_tp + u], edge_recv.at[1], sp=down, tp=u)
        for u in range(n_tp)
    ]

    @pl.when(y == SIDE - 1)
    def _():
        for copy in ctx_up:
            copy.start()

    @pl.when(y == 0)
    def _():
        for copy in ctx_down:
            copy.start()

    @pl.when(t == n_tp - 1)
    def _():
        for copy in lat_up:
            copy.start()

    @pl.when(t == 0)
    def _():
        for copy in lat_down:
            copy.start()

    weight_moves = []
    for i, (src, dst) in enumerate(pairs):
        for k in range(1, n_dp):
            at = i * n_dp + k
            weight_moves.append(
                remote(src, places[i], dp_send.at[at], dp_recv.at[at], dp=lax.rem(d + k, n_dp))
            )
            weight_moves[-1].start()

    def normed(v):
        return v * lax.rsqrt(jnp.mean(v * v, axis=1, keepdims=True) + EPSILON)

    line_wait(part_z, 0)
    summed = partial
    for k in range(1, SIDE):
        summed = summed + part_z[k - 1].astype(F32)
    part_up[...] = summed.astype(BF16)
    line(part_up, part_y, on_y, 1)

    for copy in lat_moves:
        copy.wait()
    for u in range(n_tp):
        pre[u * own_rows : (u + 1) * own_rows] = normed(lat_all[u].astype(F32))
    for k in range(1, SIDE):
        remote(context, ctx_buf.at[y], ctx_send.at[k], ctx_recv.at[k], sp=on_y(k)).wait()
    for j in range(0, SIDE, 2):
        pre[rows + PAD + j * own_ctx : rows + PAD + (j + 2) * own_ctx] = normed(
            ctx_buf[j : j + 2].astype(F32).reshape(2 * own_ctx, width)
        )
    ctx_up[0].wait_recv()
    ctx_down[0].wait_recv()
    lat_up[0].wait_recv()
    lat_down[0].wait_recv()
    pre[rows : rows + PAD] = normed(
        jnp.concatenate([halo[0], halo[1], halo[2], halo[3], jnp.zeros((PAD - 4, width), F32)], axis=0)
    )

    line_wait(part_y, 1)
    for k in range(1, SIDE):
        summed = summed + part_y[k - 1].astype(F32)
    mods[t] = summed
    moves = []
    for k in range(1, n_tp):
        moves.append(
            remote(mods.at[t], mods.at[t], mod_send.at[k], mod_recv.at[k], tp=lax.rem(t + k, n_tp))
        )
        moves[-1].start()
    for copy in small:
        copy.wait()
    for copy in moves:
        copy.wait()

    def vector(row):
        return jnp.concatenate([mods[c][row : row + 1] for c in range(n_tp)], axis=1)

    gain_row = row_of(gain)
    lat_shift, ctx_shift = vector(0), vector(1)
    lat_gain = gain_row * (1.0 + vector(2))
    ctx_gain = gain_row * (1.0 + vector(3))
    for u in range(n_tp):
        cut = slice(u * own_rows, (u + 1) * own_rows)
        hid[cut] = (pre[cut] * lat_gain + lat_shift).astype(BF16)
    at_row = lax.broadcasted_iota(jnp.int32, (PAD, width), 0)
    edge = pre[rows : rows + PAD]
    hid[rows : rows + PAD] = jnp.where(
        at_row < 2, edge * lat_gain + lat_shift, edge * ctx_gain + ctx_shift
    ).astype(BF16)
    hid[rows + PAD : rows + PAD + ctx_rows] = (
        pre[rows + PAD : rows + PAD + ctx_rows] * ctx_gain + ctx_shift
    ).astype(BF16)
    for copy in weight_moves:
        copy.wait()
    for copy in weight_copies:
        copy.wait()

    def shaped(values, before, after, taps, has_before=s > 0, has_after=s < n_sp - 1):
        count = values.shape[0]
        at = lax.broadcasted_iota(jnp.int32, values.shape, 0)
        before = jnp.where(has_before, before, 0.0)
        after = jnp.where(has_after, after, 0.0)
        earlier = jnp.where(at == 0, before, pltpu.roll(values, 1, 0))
        later = jnp.where(at == count - 1, after, pltpu.roll(values, count - 1, 0))
        w = taps[...].astype(F32)
        return silu(earlier * w[0:1] + values * w[1:2] + later * w[2:3]).astype(BF16)

    def project(weight, count):
        return dot(hid[0:count], weight[...]).astype(BF16).astype(F32)

    total = rows + PAD + ctx_rows
    spread_at = lax.broadcasted_iota(jnp.int32, (LANES, both), 0)
    spread_to = lax.broadcasted_iota(jnp.int32, (LANES, both), 1) // head_dim
    spreader = jnp.where((spread_to == spread_at) | (spread_to + nh2 == spread_at), 1.0, 0.0).astype(BF16)

    def expand(v):
        lane = lax.broadcasted_iota(jnp.int32, v.shape, 1)
        high = v.astype(BF16).astype(F32)
        low = pltpu.roll(v - high, nh2, 1)
        packed = jnp.where(lane < nh2, high, jnp.where(lane < 2 * nh2, low, 0.0))
        return dot(packed.astype(BF16), spreader)

    def running(steps):
        count = steps.shape[0]
        logs = -rates * steps
        a = lax.broadcasted_iota(jnp.int32, (count, count), 0)
        b = lax.broadcasted_iota(jnp.int32, (count, count), 1)
        lower = jnp.where(a >= b, 1.0, 0.0)
        upper = jnp.where(a <= b, 1.0, 0.0)
        lane = lax.broadcasted_iota(jnp.int32, logs.shape, 1)
        sums = jnp.where(
            lane < heads,
            dot(lower, logs, precision=lax.Precision.HIGHEST),
            dot(upper, logs, precision=lax.Precision.HIGHEST),
        )
        row_lane = lax.broadcasted_iota(jnp.int32, (1, LANES), 1)
        ends = jnp.where(row_lane < heads, sums[count - 1 : count], sums[0:1])
        return sums, ends

    def moved(values, steps):
        wide = jnp.concatenate([values, values], axis=1)
        return (wide * expand(steps)).astype(BF16)

    def spread_out(src, dst, phase):
        for a, b in far_first():
            to = lax.rem(z + a, SIDE) * SIDE + lax.rem(y + b, SIDE)
            remote(src.at[to], dst.at[s], flat_send.at[phase], flat_recv.at[phase], sp=to).start()
        dst[s] = src[s]

    def all_in(dst, phase):
        most = dst.at[pl.ds(0, n_sp - 1)]
        pltpu.make_async_copy(most, most, flat_recv.at[phase]).wait()

    def tiles(dst, state):
        for a in range(SIDE):
            for b in range(SIDE):
                dst[a * SIDE + b] = state[
                    b * TILE : (b + 1) * TILE, a * LANES : (a + 1) * LANES
                ].astype(BF16)

    features = None
    half = wd.shape[3]
    for r in range(n_dp):
        taps = jnp.concatenate(
            [wd[r, 0].astype(F32), wd[r, 1].astype(F32), jnp.zeros((LANES - nh2, half), F32)], axis=0
        ).astype(BF16)
        one = dot(hid[0:total, r * half : (r + 1) * half], taps, ((1,), (1,)))
        features = one if features is None else features + one
    step_all = softplus(features.astype(BF16).astype(F32))
    rates = jnp.concatenate([rate[0:1], rate[1:2], jnp.zeros((1, LANES - nh2), F32)], axis=1)
    c_steps = step_all[rows + PAD :]
    c_sums, c_ends = running(c_steps)
    l_steps = step_all[0:rows]
    l_sums, l_ends = running(l_steps)
    ends = expand(jnp.exp(jnp.concatenate([c_ends, l_ends, jnp.zeros((6, LANES), F32)], axis=0)))
    for a in range(SIDE):
        lanes = ends[1:2, a * LANES : (a + 1) * LANES]
        for b in range(SIDE):
            snd_t[a * SIDE + b] = lanes
    spread_out(snd_t, rcv_t, 0)

    px = project(wx, total)
    pb = project(wb, total)
    x_in = shaped(px[0:rows], px[rows : rows + 1], px[rows + 1 : rows + 2], conv_x).astype(F32)
    b_in = shaped(pb[0:rows], pb[rows : rows + 1], pb[rows + 1 : rows + 2], conv_b)
    l_moved = moved(x_in, l_steps)
    l_scaled = (l_moved.astype(F32) * expand(jnp.exp(l_ends - l_sums))).astype(BF16)
    tiles(snd_l, dot(b_in, l_scaled, ((0,), (0,))))
    spread_out(snd_l, rcv_l, 1)

    c_edges = (z > 0, z < SIDE - 1)
    cx_in = shaped(
        px[rows + PAD :], px[rows + 2 : rows + 3], px[rows + 3 : rows + 4], conv_x, *c_edges
    ).astype(F32)
    cb_in = shaped(pb[rows + PAD :], pb[rows + 2 : rows + 3], pb[rows + 3 : rows + 4], conv_b, *c_edges)
    c_moved = moved(cx_in, c_steps)
    c_scaled = (c_moved.astype(F32) * expand(jnp.exp(c_ends - c_sums))).astype(BF16)
    c_full[...] = dot(cb_in, c_scaled, ((0,), (0,)))
    c_rows = c_full[pl.ds(pl.multiple_of(y * TILE, TILE), TILE)]
    for a in range(SIDE):
        cut = slice(a * LANES, (a + 1) * LANES)
        snd_c[a, 0:TILE] = c_rows[:, cut]
        snd_c[a, TILE : TILE + 8] = jnp.broadcast_to(ends[0:1, cut], (8, LANES))
    for k in range(1, SIDE):
        to = lax.rem(z + k, SIDE)
        remote(snd_c.at[to], rcv_c.at[z], line_send.at[2], line_recv.at[2], sp=on_z(k)).start()
    rcv_c[z] = snd_c[z]

    pc = project(wc, rows + PAD)
    c_in = shaped(pc[0:rows], pc[rows : rows + 1], pc[rows + 1 : rows + 2], conv_c)
    scores = dot(c_in, b_in, ((1,), (1,)))
    at_t = lax.broadcasted_iota(jnp.int32, (rows, rows), 0)
    at_s = lax.broadcasted_iota(jnp.int32, (rows, rows), 1)
    sums_t = jnp.transpose(l_sums)

    def weights(lane, keep):
        gap = l_sums[:, lane : lane + 1] - sums_t[lane : lane + 1]
        return jnp.where(keep, scores * jnp.exp(jnp.minimum(gap, 0.0)), 0.0).astype(BF16)

    pair = LANES // head_dim
    inside = []
    lane_head = lax.broadcasted_iota(jnp.int32, (rows, LANES), 1) // head_dim
    for p in range(heads // pair):
        cut = slice(p * LANES, (p + 1) * LANES)
        cut_b = slice(inner + p * LANES, inner + (p + 1) * LANES)
        sources = jnp.concatenate([l_moved[:, cut], l_moved[:, cut_b]], axis=0)
        value = None
        for i in range(pair):
            h = p * pair + i
            w = jnp.concatenate([weights(h, at_t >= at_s), weights(heads + h, at_t <= at_s)], axis=1)
            one = dot(w, sources)
            value = one if value is None else jnp.where(lane_head == i, one, value)
        inside.append(value)
    inside = jnp.concatenate(inside, axis=1)
    growth = expand(jnp.exp(l_sums))
    gate = silu(project(wz, rows))

    forward = z < SIDE // 2

    def place(j, count=n_sp):
        return jnp.where(forward, j, count - 1 - j)

    all_in(rcv_t, 0)
    line_wait(rcv_c.at[pl.ds(0, SIDE - 1)], 2)
    state = jnp.zeros((TILE, LANES), F32)
    for j in range(SIDE):
        i = place(j, SIDE)
        state = state * rcv_c[i, TILE : TILE + 1] + rcv_c[i, 0:TILE]
    all_in(rcv_l, 1)

    def latent_step(j, state):
        i = place(j)
        snd_b[i] = state.astype(BF16)
        return state * rcv_t[i] + rcv_l[i].astype(F32)

    lax.fori_loop(0, n_sp, latent_step, state, unroll=8)
    spread_out(snd_b, rcv_b, 2)
    all_in(rcv_b, 2)
    entering = jnp.concatenate(
        [rcv_b[a * SIDE : (a + 1) * SIDE].reshape(STATE, LANES) for a in range(SIDE)], axis=1
    )
    carried = dot(c_in, entering) * growth
    gated = (inside + carried[:, 0:inner] + carried[:, inner:both]) * gate
    ny = (
        gated
        * lax.rsqrt(jnp.mean(gated * gated, axis=1, keepdims=True) + EPSILON)
        * row_of(out_gain)
    ).astype(BF16)

    chunks = n_tp
    chunk = width // chunks
    o_moves = []
    for c in range(chunks):
        cut = slice(c * chunk, (c + 1) * chunk)
        result = dot(ny, wo[:, cut]).astype(BF16)
        for u in range(n_tp):
            snd_o[c, u] = result[u * own_rows : (u + 1) * own_rows]
        for k in range(1, n_tp):
            to = lax.rem(t + k, n_tp)
            at = c * n_tp + k
            o_moves.append(remote(snd_o.at[c, to], rcv_o.at[c, k], o_send.at[at], o_recv.at[at], tp=to))
            o_moves[-1].start()

    for phase, sent in ((0, part_z), (1, part_y), (2, rcv_c.at[pl.ds(0, SIDE - 1)])):
        pltpu.make_async_copy(sent, sent, line_send.at[phase]).wait()
    for phase, sent in ((0, rcv_t), (1, rcv_l), (2, rcv_b)):
        most = sent.at[pl.ds(0, n_sp - 1)]
        pltpu.make_async_copy(most, most, flat_send.at[phase]).wait()

    @pl.when(y == SIDE - 1)
    def _():
        for copy in ctx_up:
            copy.wait_send()

    @pl.when(y == 0)
    def _():
        for copy in ctx_down:
            copy.wait_send()

    @pl.when(t == n_tp - 1)
    def _():
        for copy in lat_up:
            copy.wait_send()

    @pl.when(t == 0)
    def _():
        for copy in lat_down:
            copy.wait_send()

    for c in range(chunks):
        mixed = snd_o[c, t].astype(F32)
        for k in range(1, n_tp):
            o_moves[c * (n_tp - 1) + k - 1].wait()
            mixed = mixed + rcv_o[c, k].astype(F32)
        out[:, c * chunk : (c + 1) * chunk] = (mods[c][4:5] * mixed).astype(BF16)


def shards(
    latent,
    condition,
    context,
    context_source,
    mod_weight,
    norm_gain,
    w_x,
    w_b,
    w_c,
    w_z,
    w_dt,
    conv_x,
    conv_b,
    conv_c,
    decay_rate,
    out_gain,
    w_out,
):
    n_sp, n_tp, n_dp = lax.axis_size("sp"), lax.axis_size("tp"), lax.axis_size("dp")
    assert n_sp == SIDE * SIDE
    own_rows, width = latent.shape[1:]
    own_ctx = context.shape[1]
    ctx_rows = SIDE * own_ctx
    cols = mod_weight.shape[2]
    inner = w_x.shape[1]
    heads = decay_rate.shape[1]
    assert STATE == SIDE * TILE and 2 * inner == SIDE * LANES
    rows = n_tp * own_rows
    total = rows + PAD + ctx_rows
    chunk = width // n_tp
    vmem = pl.BlockSpec(memory_space=pltpu.VMEM)
    anywhere = pl.BlockSpec(memory_space=pl.ANY)
    dma = pltpu.SemaphoreType.DMA
    args = (
        condition,
        context_source,
        norm_gain,
        conv_x,
        conv_b,
        conv_c,
        decay_rate,
        out_gain,
        latent[0],
        context[0],
        mod_weight,
        w_x,
        w_b,
        w_c,
        jnp.swapaxes(w_dt, 1, 2),
        w_z,
        w_out,
    )
    tiles = pltpu.VMEM((n_sp, TILE, LANES), BF16)
    scratch = [pltpu.VMEM(a.shape, a.dtype) for a in args[:8]] + [
        pltpu.VMEM((n_tp, own_rows, width), BF16),
        pltpu.VMEM((SIDE, own_ctx, width), BF16),
        pltpu.VMEM(mod_weight.shape, BF16),
        pltpu.VMEM((w_x.shape[0] * n_dp, inner), BF16),
        pltpu.VMEM((w_b.shape[0] * n_dp, w_b.shape[1]), BF16),
        pltpu.VMEM((w_c.shape[0] * n_dp, w_c.shape[1]), BF16),
        pltpu.VMEM((n_dp, 2, heads, w_dt.shape[1]), BF16),
        pltpu.VMEM((w_z.shape[0] * n_dp, inner), BF16),
        pltpu.VMEM((w_out.shape[0] * n_dp, width), BF16),
        pltpu.VMEM((8, width), F32),
        pltpu.VMEM((4, 1, width), F32),
        pltpu.VMEM((8, cols), BF16),
        pltpu.VMEM((SIDE - 1, 8, cols), BF16),
        pltpu.VMEM((8, cols), BF16),
        pltpu.VMEM((SIDE - 1, 8, cols), BF16),
        pltpu.VMEM((n_tp, 8, cols), F32),
        pltpu.VMEM((4, 1, width), F32),
        pltpu.VMEM((total, width), F32),
        pltpu.VMEM((total, width), BF16),
        pltpu.VMEM((STATE, 2 * inner), F32),
        pltpu.VMEM((SIDE, TILE + 8, LANES), F32),
        pltpu.VMEM((SIDE, TILE + 8, LANES), F32),
        tiles,
        tiles,
        pltpu.VMEM((n_sp, 1, LANES), F32),
        pltpu.VMEM((n_sp, 1, LANES), F32),
        tiles,
        tiles,
        pltpu.VMEM((n_tp, n_tp, own_rows, chunk), BF16),
        pltpu.VMEM((n_tp, n_tp, own_rows, chunk), BF16),
        dma((17,)),
        dma((6 * n_dp,)),
        dma((6 * n_dp,)),
        dma((n_tp,)),
        dma((n_tp,)),
        dma((3,)),
        dma((3,)),
        dma((n_tp,)),
        dma((n_tp,)),
        dma((SIDE,)),
        dma((SIDE,)),
        dma((2 * SIDE + 2 * n_tp,)),
        dma((4,)),
        dma((3,)),
        dma((3,)),
        dma((n_tp * n_tp,)),
        dma((n_tp * n_tp,)),
    ]
    result = pl.pallas_call(
        functools.partial(kernel, n_sp, n_tp, n_dp, heads),
        out_shape=pltpu.VMEM((own_rows, width), BF16),
        in_specs=[anywhere] * len(args),
        out_specs=vmem,
        scratch_shapes=scratch,
        compiler_params=pltpu.CompilerParams(
            collective_id=0, has_side_effects=True, vmem_limit_bytes=62_000_000
        ),
    )(*args)
    return result[None]


def solution(mesh):
    placed = (
        P("dp", ("sp", "tp"), None),
        P("dp", None),
        P("dp", "sp", None),
        P(),
        P(None, "sp", "tp"),
        P(),
        P("dp", "tp"),
        P("dp", "tp"),
        P("dp", "tp"),
        P("dp", "tp"),
        P(None, "dp", "tp"),
        P(None, "tp"),
        P(None, "tp"),
        P(None, "tp"),
        P(None, "tp"),
        P("tp"),
        P(("tp", "dp"), None),
    )
    return jax.shard_map(
        shards, mesh=mesh, in_specs=placed, out_specs=P("dp", ("sp", "tp"), None), check_vma=False
    )
```

```python
import functools

import jax
import jax.numpy as jnp
from jax import lax
from jax.experimental import pallas as pl
from jax.experimental.pallas import tpu as pltpu
from jax.sharding import PartitionSpec as P

STATE = 128
LANES = 128
PAD = 16
SIDE = 8
TILE = 16
EPSILON = 1e-06
MESH = pl.DeviceIdType.MESH
F32 = jnp.float32
BF16 = jnp.bfloat16


def silu(v):
    return v / (1.0 + jnp.exp(-v))


def softplus(v):
    return jnp.maximum(v, 0.0) + jnp.log1p(jnp.exp(-jnp.abs(v)))


def row_of(ref):
    return ref[...].astype(F32).reshape(1, ref.shape[0])


def dot(a, b, dims=((1,), (0,)), precision=None):
    return lax.dot_general(a, b, (dims, ((), ())), precision=precision, preferred_element_type=F32)


def far_first():
    def reach(k):
        return min(k, SIDE - k)

    steps = [(a, b) for a in range(SIDE) for b in range(SIDE) if a or b]
    return sorted(steps, key=lambda ab: -(reach(ab[0]) + reach(ab[1])))


def kernel(
    n_sp,
    n_tp,
    n_dp,
    heads,
    condition_in,
    source_in,
    gain_in,
    conv_x_in,
    conv_b_in,
    conv_c_in,
    rate_in,
    out_gain_in,
    latent,
    context,
    mod_weight,
    w_x,
    w_b,
    w_c,
    w_dt,
    w_z,
    w_out,
    out,
    condition,
    source,
    gain,
    conv_x,
    conv_b,
    conv_c,
    rate,
    out_gain,
    lat_all,
    ctx_buf,
    mod_buf,
    wx,
    wb,
    wc,
    wd,
    wz,
    wo,
    acts,
    edges,
    part,
    part_z,
    part_up,
    part_y,
    mods,
    halo,
    pre,
    hid,
    c_full,
    snd_c,
    rcv_c,
    snd_l,
    rcv_l,
    snd_t,
    rcv_t,
    snd_b,
    rcv_b,
    snd_o,
    rcv_o,
    weights_like,
    local_sem,
    weight_sem,
    pack_sem,
    line_send,
    line_recv,
    edge_sem,
    flat_send,
    flat_recv,
    o_sem,
):
    s = lax.axis_index("sp")
    t = lax.axis_index("tp")
    d = lax.axis_index("dp")
    z = s // SIDE
    y = lax.rem(s, SIDE)
    own_rows, width = latent.shape
    own_ctx = context.shape[0]
    ctx_rows = SIDE * own_ctx
    depth = mod_weight.shape[1]
    rows = n_tp * own_rows
    inner = w_x.shape[1]
    both = 2 * inner
    head_dim = inner // heads
    nh2 = 2 * heads
    up, down = lax.rem(s + 1, n_sp), lax.rem(s + n_sp - 1, n_sp)

    def remote(src, dst, send, recv, **to):
        return pltpu.make_async_remote_copy(
            src_ref=src, dst_ref=dst, send_sem=send, recv_sem=recv, device_id=to, device_id_type=MESH
        )

    barrier = pltpu.get_barrier_semaphore()

    def greet(**to):
        pl.semaphore_signal(barrier, inc=1, device_id=to, device_id_type=MESH)

    def on_z(k):
        return lax.rem(z + k, SIDE) * SIDE + y

    def on_y(k):
        return z * SIDE + lax.rem(y + k, SIDE)

    for k in range(1, SIDE):
        greet(sp=on_z(k))
        greet(sp=on_y(k))
    for k in range(1, n_tp):
        greet(tp=lax.rem(t + k, n_tp))
    for k in range(1, n_dp):
        greet(dp=lax.rem(d + k, n_dp))
    z_up, z_down = lax.rem(z + 1, SIDE) * SIDE, lax.rem(z + SIDE - 1, SIDE) * SIDE
    greet(sp=z_down + SIDE - 1)
    greet(sp=z_up)
    greet(sp=down, tp=n_tp - 1)
    greet(sp=up, tp=0)

    local = []

    def fetch(src, dst):
        copy = pltpu.make_async_copy(src, dst, local_sem.at[len(local)])
        copy.start()
        local.append(copy)
        return copy

    def settle(ref, sem):
        pltpu.make_async_copy(ref, ref, sem).wait()

    early = [fetch(condition_in, condition), fetch(source_in, source), fetch(mod_weight, mod_buf)]
    lat_copy = fetch(latent, lat_all.at[t])
    ctx_copy = fetch(context, ctx_buf.at[y])
    small = [
        fetch(a, b)
        for a, b in (
            (gain_in, gain),
            (conv_x_in, conv_x),
            (conv_b_in, conv_b),
            (conv_c_in, conv_c),
            (rate_in, rate),
            (out_gain_in, out_gain),
        )
    ]
    pairs = ((w_x, wx), (w_b, wb), (w_dt, wd), (w_c, wc), (w_z, wz), (w_out, wo))
    places = []
    for src, dst in pairs:
        count = src.shape[0]
        places.append(dst.at[d] if src is w_dt else dst.at[pl.ds(d * count, count)])
        pltpu.make_async_copy(src, places[-1], weight_sem.at[0]).start()

    for copy in early:
        copy.wait()
    acts[0:1] = condition[...].astype(F32)
    acts[1:2] = row_of(source)
    per = LANES // depth
    block = acts[0:2, pl.ds(pl.multiple_of((s // per) * LANES, LANES), LANES)]
    active = jnp.concatenate([silu(block), jnp.zeros((PAD - 2, LANES), F32)], axis=0)
    own_acts = active[:, 0:depth]
    for j in range(1, per):
        own_acts = jnp.where(lax.rem(s, per) == j, active[:, j * depth : (j + 1) * depth], own_acts)
    own_acts = own_acts.astype(BF16)
    pieces = [dot(own_acts, mod_buf[k])[0:2] for k in range(mod_buf.shape[0])]
    cols = pieces[0].shape[1]

    def packed(rows_f32):
        low = [rows_f32[r : r + 1] - rows_f32[r : r + 1].astype(BF16).astype(F32) for r in (0, 2, 4)]
        return jnp.concatenate([rows_f32[0:5]] + low, axis=0).astype(BF16)

    def unpacked(total):
        fine = [total[r : r + 1] + total[5 + r // 2 : 6 + r // 2] for r in (0, 2, 4)]
        return jnp.concatenate(
            [fine[0], total[1:2], fine[1], total[3:4], fine[2], jnp.zeros((3, cols), F32)], axis=0
        )

    partial = jnp.concatenate(pieces + [jnp.zeros((2, cols), F32)], axis=0)
    part[...] = packed(partial)

    lat_copy.wait()
    edges[0] = lat_all[t, 0:1].astype(F32)
    edges[1] = lat_all[t, own_rows - 1 : own_rows].astype(F32)
    ctx_copy.wait()
    edges[2] = ctx_buf[y, 0:1].astype(F32)
    edges[3] = ctx_buf[y, own_ctx - 1 : own_ctx].astype(F32)

    expected = 2 * (SIDE - 1) + n_tp - 1 + n_dp - 1
    expected = expected + jnp.where(y == SIDE - 1, SIDE, 0) + jnp.where(y == 0, SIDE, 0)
    expected = expected + jnp.where(t == n_tp - 1, n_tp, 0) + jnp.where(t == 0, n_tp, 0)
    pl.semaphore_wait(barrier, expected)

    def line(src, dst, place, phase):
        for k in range(1, SIDE):
            remote(src, dst.at[k - 1], line_send.at[phase], line_recv.at[phase], sp=place(k)).start()

    def line_wait(dst, phase):
        pltpu.make_async_copy(dst, dst, line_recv.at[phase]).wait()

    line(part, part_z, on_z, 0)
    for k in range(1, n_tp):
        remote(latent, lat_all.at[t], pack_sem.at[0], pack_sem.at[1], tp=lax.rem(t + k, n_tp)).start()
    ctx_up = [
        remote(edges.at[3], halo.at[2], edge_sem.at[0], edge_sem.at[4], sp=z_up + j) for j in range(SIDE)
    ]
    ctx_down = [
        remote(edges.at[2], halo.at[3], edge_sem.at[1], edge_sem.at[4], sp=z_down + j)
        for j in range(SIDE)
    ]
    lat_up = [
        remote(edges.at[1], halo.at[0], edge_sem.at[2], edge_sem.at[4], sp=up, tp=u)
        for u in range(n_tp)
    ]
    lat_down = [
        remote(edges.at[0], halo.at[1], edge_sem.at[3], edge_sem.at[4], sp=down, tp=u)
        for u in range(n_tp)
    ]

    @pl.when(y == SIDE - 1)
    def _():
        for copy in ctx_up:
            copy.start()

    @pl.when(y == 0)
    def _():
        for copy in ctx_down:
            copy.start()

    @pl.when(t == n_tp - 1)
    def _():
        for copy in lat_up:
            copy.start()

    @pl.when(t == 0)
    def _():
        for copy in lat_down:
            copy.start()

    for i, (src, dst) in enumerate(pairs):
        remote(src, places[i], weight_sem.at[1], weight_sem.at[2], dp=1 - d).start()

    def normed(v):
        return v * lax.rsqrt(jnp.mean(v * v, axis=1, keepdims=True) + EPSILON)

    line_wait(part_z, 0)
    others = part_z[0].astype(F32)
    for k in range(2, SIDE):
        others = others + part_z[k - 1].astype(F32)
    summed = partial + unpacked(others)
    part_up[...] = packed(summed)
    line(part_up, part_y, on_y, 1)
    for k in range(1, SIDE):
        remote(ctx_buf.at[y], ctx_buf.at[y], pack_sem.at[2], pack_sem.at[3], sp=on_y(k)).start()

    line_wait(part_y, 1)
    others = part_y[0].astype(F32)
    for k in range(2, SIDE):
        others = others + part_y[k - 1].astype(F32)
    mods[t] = summed + unpacked(others)
    for k in range(1, n_tp):
        remote(mods.at[t], mods.at[t], pack_sem.at[4], pack_sem.at[5], tp=lax.rem(t + k, n_tp)).start()
    settle(lat_all.at[pl.ds(0, n_tp - 1)], pack_sem.at[1])
    for u in range(n_tp):
        pre[u * own_rows : (u + 1) * own_rows] = normed(lat_all[u].astype(F32))
    settle(ctx_buf.at[pl.ds(0, SIDE - 1)], pack_sem.at[3])
    for j in range(0, SIDE, 2):
        pre[rows + PAD + j * own_ctx : rows + PAD + (j + 2) * own_ctx] = normed(
            ctx_buf[j : j + 2].astype(F32).reshape(2 * own_ctx, width)
        )
    settle(halo, edge_sem.at[4])
    pre[rows : rows + PAD] = normed(
        jnp.concatenate([halo[0], halo[1], halo[2], halo[3], jnp.zeros((PAD - 4, width), F32)], axis=0)
    )

    for copy in small:
        copy.wait()
    settle(mods.at[pl.ds(0, n_tp - 1)], pack_sem.at[5])

    def vector(row):
        return jnp.concatenate([mods[c][row : row + 1] for c in range(n_tp)], axis=1)

    gain_row = row_of(gain)
    lat_shift, ctx_shift = vector(0), vector(1)
    lat_gain = gain_row * (1.0 + vector(2))
    ctx_gain = gain_row * (1.0 + vector(3))
    for u in range(n_tp):
        cut = slice(u * own_rows, (u + 1) * own_rows)
        hid[cut] = (pre[cut] * lat_gain + lat_shift).astype(BF16)
    at_row = lax.broadcasted_iota(jnp.int32, (PAD, width), 0)
    edge = pre[rows : rows + PAD]
    hid[rows : rows + PAD] = jnp.where(
        at_row < 2, edge * lat_gain + lat_shift, edge * ctx_gain + ctx_shift
    ).astype(BF16)
    hid[rows + PAD : rows + PAD + ctx_rows] = (
        pre[rows + PAD : rows + PAD + ctx_rows] * ctx_gain + ctx_shift
    ).astype(BF16)
    settle(weights_like, weight_sem.at[0])
    settle(weights_like, weight_sem.at[2])

    def shaped(values, before, after, taps, has_before=s > 0, has_after=s < n_sp - 1):
        count = values.shape[0]
        at = lax.broadcasted_iota(jnp.int32, values.shape, 0)
        before = jnp.where(has_before, before, 0.0)
        after = jnp.where(has_after, after, 0.0)
        earlier = jnp.where(at == 0, before, pltpu.roll(values, 1, 0))
        later = jnp.where(at == count - 1, after, pltpu.roll(values, count - 1, 0))
        w = taps[...].astype(F32)
        return silu(earlier * w[0:1] + values * w[1:2] + later * w[2:3]).astype(BF16)

    def project(weight, count):
        return dot(hid[0:count], weight[...]).astype(BF16).astype(F32)

    total = rows + PAD + ctx_rows
    spread_at = lax.broadcasted_iota(jnp.int32, (LANES, both), 0)
    spread_to = lax.broadcasted_iota(jnp.int32, (LANES, both), 1) // head_dim
    spreader = jnp.where((spread_to == spread_at) | (spread_to + nh2 == spread_at), 1.0, 0.0).astype(BF16)

    def expand(v):
        lane = lax.broadcasted_iota(jnp.int32, v.shape, 1)
        high = v.astype(BF16).astype(F32)
        low = pltpu.roll(v - high, nh2, 1)
        packed = jnp.where(lane < nh2, high, jnp.where(lane < 2 * nh2, low, 0.0))
        return dot(packed.astype(BF16), spreader)

    def running(steps):
        count = steps.shape[0]
        logs = -rates * steps
        high = logs.astype(BF16).astype(F32)
        rest = logs - high
        middle = rest.astype(BF16).astype(F32)
        low = rest - middle
        packed = high + pltpu.roll(middle, nh2, 1) + pltpu.roll(low, 2 * nh2, 1)
        a = lax.broadcasted_iota(jnp.int32, (2 * count, count), 0)
        b = lax.broadcasted_iota(jnp.int32, (2 * count, count), 1)
        keep = jnp.where(a < count, jnp.where(a >= b, 1.0, 0.0), jnp.where(a - count <= b, 1.0, 0.0))
        parts = dot(keep.astype(BF16), packed.astype(BF16))
        lane = lax.broadcasted_iota(jnp.int32, (count, LANES), 1)
        parts = jnp.where(lax.rem(lane, nh2) < heads, parts[0:count], parts[count:])
        sums = parts + pltpu.roll(parts, LANES - nh2, 1) + pltpu.roll(parts, LANES - 2 * nh2, 1)
        sums = jnp.where(lane < nh2, sums, 0.0)
        row_lane = lax.broadcasted_iota(jnp.int32, (1, LANES), 1)
        ends = jnp.where(row_lane < heads, sums[count - 1 : count], sums[0:1])
        return sums, ends

    def moved(values, steps):
        wide = jnp.concatenate([values, values], axis=1)
        return (wide * expand(steps)).astype(BF16)

    def spread_out(src, dst, phase):
        for a, b in far_first():
            to = lax.rem(z + a, SIDE) * SIDE + lax.rem(y + b, SIDE)
            remote(src.at[to], dst.at[s], flat_send.at[phase], flat_recv.at[phase], sp=to).start()
        dst[s] = src[s]

    def all_in(dst, phase):
        most = dst.at[pl.ds(0, n_sp - 1)]
        pltpu.make_async_copy(most, most, flat_recv.at[phase]).wait()

    def tiles(dst, state):
        for a in range(SIDE):
            for b in range(SIDE):
                dst[a * SIDE + b] = state[
                    b * TILE : (b + 1) * TILE, a * LANES : (a + 1) * LANES
                ].astype(BF16)

    features = None
    half = wd.shape[3]
    for r in range(n_dp):
        taps = jnp.concatenate(
            [wd[r, 0].astype(F32), wd[r, 1].astype(F32), jnp.zeros((LANES - nh2, half), F32)], axis=0
        ).astype(BF16)
        one = dot(hid[0:total, r * half : (r + 1) * half], taps, ((1,), (1,)))
        features = one if features is None else features + one
    step_all = softplus(features.astype(BF16).astype(F32))
    rates = jnp.concatenate([rate[0:1], rate[1:2], jnp.zeros((1, LANES - nh2), F32)], axis=1)
    c_steps = step_all[rows + PAD :]
    c_sums, c_ends = running(c_steps)
    l_steps = step_all[0:rows]
    l_sums, l_ends = running(l_steps)
    ends = expand(jnp.exp(jnp.concatenate([c_ends, l_ends, jnp.zeros((6, LANES), F32)], axis=0)))
    for a in range(SIDE):
        lanes = ends[1:2, a * LANES : (a + 1) * LANES]
        for b in range(SIDE):
            snd_t[a * SIDE + b] = lanes
    px = project(wx, total)
    pb = project(wb, total)
    x_in = shaped(px[0:rows], px[rows : rows + 1], px[rows + 1 : rows + 2], conv_x).astype(F32)
    b_in = shaped(pb[0:rows], pb[rows : rows + 1], pb[rows + 1 : rows + 2], conv_b)
    l_moved = moved(x_in, l_steps)
    l_scaled = (l_moved.astype(F32) * expand(jnp.exp(l_ends - l_sums))).astype(BF16)
    tiles(snd_l, dot(b_in, l_scaled, ((0,), (0,))))
    spread_out(snd_l, rcv_l, 1)
    spread_out(snd_t, rcv_t, 0)

    c_edges = (z > 0, z < SIDE - 1)
    cx_in = shaped(
        px[rows + PAD :], px[rows + 2 : rows + 3], px[rows + 3 : rows + 4], conv_x, *c_edges
    ).astype(F32)
    cb_in = shaped(pb[rows + PAD :], pb[rows + 2 : rows + 3], pb[rows + 3 : rows + 4], conv_b, *c_edges)
    c_moved = moved(cx_in, c_steps)
    c_scaled = (c_moved.astype(F32) * expand(jnp.exp(c_ends - c_sums))).astype(BF16)
    c_full[...] = dot(cb_in, c_scaled, ((0,), (0,)))
    c_rows = c_full[pl.ds(pl.multiple_of(y * TILE, TILE), TILE)]
    for a in range(SIDE):
        cut = slice(a * LANES, (a + 1) * LANES)
        snd_c[a, 0:TILE] = c_rows[:, cut]
        snd_c[a, TILE : TILE + 8] = jnp.broadcast_to(ends[0:1, cut], (8, LANES))
    for k in range(1, SIDE):
        to = lax.rem(z + k, SIDE)
        remote(snd_c.at[to], rcv_c.at[z], line_send.at[2], line_recv.at[2], sp=on_z(k)).start()
    rcv_c[z] = snd_c[z]

    pc = project(wc, rows + PAD)
    c_in = shaped(pc[0:rows], pc[rows : rows + 1], pc[rows + 1 : rows + 2], conv_c)
    scores = dot(c_in, b_in, ((1,), (1,)))
    at_t = lax.broadcasted_iota(jnp.int32, (rows, rows), 0)
    at_s = lax.broadcasted_iota(jnp.int32, (rows, rows), 1)
    sums_t = jnp.transpose(l_sums)

    def weights(lane, keep):
        gap = l_sums[:, lane : lane + 1] - sums_t[lane : lane + 1]
        return jnp.where(keep, scores * jnp.exp(jnp.minimum(gap, 0.0)), 0.0).astype(BF16)

    pair = LANES // head_dim
    inside = []
    lane_head = lax.broadcasted_iota(jnp.int32, (rows, LANES), 1) // head_dim
    for p in range(heads // pair):
        cut = slice(p * LANES, (p + 1) * LANES)
        cut_b = slice(inner + p * LANES, inner + (p + 1) * LANES)
        sources = jnp.concatenate([l_moved[:, cut], l_moved[:, cut_b]], axis=0)
        value = None
        for i in range(pair):
            h = p * pair + i
            w = jnp.concatenate([weights(h, at_t >= at_s), weights(heads + h, at_t <= at_s)], axis=1)
            one = dot(w, sources)
            value = one if value is None else jnp.where(lane_head == i, one, value)
        inside.append(value)
    inside = jnp.concatenate(inside, axis=1)
    growth = expand(jnp.exp(l_sums))
    gate = silu(project(wz, rows))

    forward = z < SIDE // 2

    def place(j, count=n_sp):
        return jnp.where(forward, j, count - 1 - j)

    line_wait(rcv_c.at[pl.ds(0, SIDE - 1)], 2)
    state = jnp.zeros((TILE, LANES), F32)
    for j in range(SIDE):
        i = place(j, SIDE)
        state = state * rcv_c[i, TILE : TILE + 1] + rcv_c[i, 0:TILE]
    all_in(rcv_t, 0)
    all_in(rcv_l, 1)

    def latent_step(j, state):
        i = place(j)
        snd_b[i] = state.astype(BF16)
        return state * rcv_t[i] + rcv_l[i].astype(F32)

    lax.fori_loop(0, n_sp, latent_step, state, unroll=8)
    spread_out(snd_b, rcv_b, 2)
    all_in(rcv_b, 2)
    entering = jnp.concatenate(
        [rcv_b[a * SIDE : (a + 1) * SIDE].reshape(STATE, LANES) for a in range(SIDE)], axis=1
    )
    carried = dot(c_in, entering) * growth
    gated = (inside + carried[:, 0:inner] + carried[:, inner:both]) * gate
    ny = (
        gated
        * lax.rsqrt(jnp.mean(gated * gated, axis=1, keepdims=True) + EPSILON)
        * row_of(out_gain)
    ).astype(BF16)

    chunks = n_tp
    chunk = width // chunks
    far_tp = sorted(range(1, n_tp), key=lambda k: -min(k, n_tp - k))
    for c in range(chunks):
        cut = slice(c * chunk, (c + 1) * chunk)
        result = dot(ny, wo[:, cut]).astype(BF16)
        for u in range(n_tp):
            snd_o[c, u] = result[u * own_rows : (u + 1) * own_rows]
        for k in far_tp:
            to = lax.rem(t + k, n_tp)
            remote(snd_o.at[c, to], rcv_o.at[c, k - 1], o_sem.at[chunks], o_sem.at[c], tp=to).start()

    for phase, sent in ((0, part_z), (1, part_y), (2, rcv_c.at[pl.ds(0, SIDE - 1)])):
        settle(sent, line_send.at[phase])
    for phase, sent in ((0, rcv_t), (1, rcv_l), (2, rcv_b)):
        settle(sent.at[pl.ds(0, n_sp - 1)], flat_send.at[phase])
    settle(weights_like, weight_sem.at[1])
    settle(lat_all.at[pl.ds(0, n_tp - 1)], pack_sem.at[0])
    settle(ctx_buf.at[pl.ds(0, SIDE - 1)], pack_sem.at[2])
    settle(mods.at[pl.ds(0, n_tp - 1)], pack_sem.at[4])

    @pl.when(y == SIDE - 1)
    def _():
        settle(acts, edge_sem.at[0])

    @pl.when(y == 0)
    def _():
        settle(acts, edge_sem.at[1])

    @pl.when(t == n_tp - 1)
    def _():
        settle(halo, edge_sem.at[2])

    @pl.when(t == 0)
    def _():
        settle(halo, edge_sem.at[3])

    for c in range(chunks):
        mixed = snd_o[c, t].astype(F32)
        settle(rcv_o.at[c], o_sem.at[c])
        for k in range(1, n_tp):
            mixed = mixed + rcv_o[c, k - 1].astype(F32)
        out[:, c * chunk : (c + 1) * chunk] = (mods[c][4:5] * mixed).astype(BF16)
    settle(rcv_o, o_sem.at[chunks])


def shards(
    latent,
    condition,
    context,
    context_source,
    mod_weight,
    norm_gain,
    w_x,
    w_b,
    w_c,
    w_z,
    w_dt,
    conv_x,
    conv_b,
    conv_c,
    decay_rate,
    out_gain,
    w_out,
):
    n_sp, n_tp, n_dp = lax.axis_size("sp"), lax.axis_size("tp"), lax.axis_size("dp")
    assert n_sp == SIDE * SIDE
    own_rows, width = latent.shape[1:]
    own_ctx = context.shape[1]
    ctx_rows = SIDE * own_ctx
    cols = mod_weight.shape[2]
    inner = w_x.shape[1]
    heads = decay_rate.shape[1]
    assert STATE == SIDE * TILE and 2 * inner == SIDE * LANES
    rows = n_tp * own_rows
    total = rows + PAD + ctx_rows
    chunk = width // n_tp
    vmem = pl.BlockSpec(memory_space=pltpu.VMEM)
    anywhere = pl.BlockSpec(memory_space=pl.ANY)
    dma = pltpu.SemaphoreType.DMA
    args = (
        condition,
        context_source,
        norm_gain,
        conv_x,
        conv_b,
        conv_c,
        decay_rate,
        out_gain,
        latent[0],
        context[0],
        mod_weight,
        w_x,
        w_b,
        w_c,
        jnp.swapaxes(w_dt, 1, 2),
        w_z,
        w_out,
    )
    tiles = pltpu.VMEM((n_sp, TILE, LANES), BF16)
    sent_rows = sum(w.size for w in (w_x, w_b, w_c, w_dt, w_z, w_out)) // width
    scratch = [pltpu.VMEM(a.shape, a.dtype) for a in args[:8]] + [
        pltpu.VMEM((n_tp, own_rows, width), BF16),
        pltpu.VMEM((SIDE, own_ctx, width), BF16),
        pltpu.VMEM(mod_weight.shape, BF16),
        pltpu.VMEM((w_x.shape[0] * n_dp, inner), BF16),
        pltpu.VMEM((w_b.shape[0] * n_dp, w_b.shape[1]), BF16),
        pltpu.VMEM((w_c.shape[0] * n_dp, w_c.shape[1]), BF16),
        pltpu.VMEM((n_dp, 2, heads, w_dt.shape[1]), BF16),
        pltpu.VMEM((w_z.shape[0] * n_dp, inner), BF16),
        pltpu.VMEM((w_out.shape[0] * n_dp, width), BF16),
        pltpu.VMEM((8, width), F32),
        pltpu.VMEM((4, 1, width), F32),
        pltpu.VMEM((8, cols), BF16),
        pltpu.VMEM((SIDE - 1, 8, cols), BF16),
        pltpu.VMEM((8, cols), BF16),
        pltpu.VMEM((SIDE - 1, 8, cols), BF16),
        pltpu.VMEM((n_tp, 8, cols), F32),
        pltpu.VMEM((4, 1, width), F32),
        pltpu.VMEM((total, width), F32),
        pltpu.VMEM((total, width), BF16),
        pltpu.VMEM((STATE, 2 * inner), F32),
        pltpu.VMEM((SIDE, TILE + 8, LANES), F32),
        pltpu.VMEM((SIDE, TILE + 8, LANES), F32),
        tiles,
        tiles,
        pltpu.VMEM((n_sp, 1, LANES), F32),
        pltpu.VMEM((n_sp, 1, LANES), F32),
        tiles,
        tiles,
        pltpu.VMEM((n_tp, n_tp, own_rows, chunk), BF16),
        pltpu.VMEM((n_tp, n_tp - 1, own_rows, chunk), BF16),
        pltpu.VMEM((sent_rows, width), BF16),
        dma((11,)),
        dma((3,)),
        dma((6,)),
        dma((3,)),
        dma((3,)),
        dma((5,)),
        dma((3,)),
        dma((3,)),
        dma((n_tp + 1,)),
    ]
    result = pl.pallas_call(
        functools.partial(kernel, n_sp, n_tp, n_dp, heads),
        out_shape=pltpu.VMEM((own_rows, width), BF16),
        in_specs=[anywhere] * len(args),
        out_specs=vmem,
        scratch_shapes=scratch,
        compiler_params=pltpu.CompilerParams(
            collective_id=0, has_side_effects=True, vmem_limit_bytes=62_000_000
        ),
    )(*args)
    return result[None]


def solution(mesh):
    placed = (
        P("dp", ("sp", "tp"), None),
        P("dp", None),
        P("dp", "sp", None),
        P(),
        P(None, "sp", "tp"),
        P(),
        P("dp", "tp"),
        P("dp", "tp"),
        P("dp", "tp"),
        P("dp", "tp"),
        P(None, "dp", "tp"),
        P(None, "tp"),
        P(None, "tp"),
        P(None, "tp"),
        P(None, "tp"),
        P("tp"),
        P(("tp", "dp"), None),
    )
    return jax.shard_map(
        shards, mesh=mesh, in_specs=placed, out_specs=P("dp", ("sp", "tp"), None), check_vma=False
    )
```

```python
import functools

import jax
import jax.numpy as jnp
from jax import lax
from jax.experimental import pallas as pl
from jax.experimental.pallas import tpu as pltpu
from jax.sharding import PartitionSpec as P

STATE = 128
LANES = 128
PAD = 16
SIDE = 8
TILE = 16
EPSILON = 1e-06
MESH = pl.DeviceIdType.MESH
F32 = jnp.float32
BF16 = jnp.bfloat16


def silu(v):
    return v / (1.0 + jnp.exp(-v))


def softplus(v):
    return jnp.maximum(v, 0.0) + jnp.log1p(jnp.exp(-jnp.abs(v)))


def row_of(ref):
    return ref[...].astype(F32).reshape(1, ref.shape[0])


def dot(a, b, dims=((1,), (0,)), precision=None):
    return lax.dot_general(a, b, (dims, ((), ())), precision=precision, preferred_element_type=F32)


def reach(k):
    return min(k, SIDE - k)


def along():
    return sorted(range(1, SIDE), key=lambda k: -reach(k))


def far_first():
    steps = [(a, b) for a in range(SIDE) for b in range(SIDE) if a or b]
    return sorted(steps, key=lambda ab: -(reach(ab[0]) + reach(ab[1])))


def kernel(
    n_sp,
    n_tp,
    n_dp,
    heads,
    condition_in,
    source_in,
    gain_in,
    conv_x_in,
    conv_b_in,
    conv_c_in,
    rate_in,
    out_gain_in,
    latent,
    context,
    mod_weight,
    w_x,
    w_b,
    w_c,
    w_dt,
    w_z,
    w_out,
    out,
    condition,
    source,
    gain,
    conv_x,
    conv_b,
    conv_c,
    rate,
    out_gain,
    lat_all,
    ctx_buf,
    mod_buf,
    wx,
    wb,
    wc,
    wd,
    wz,
    wo,
    acts,
    edges,
    part,
    part_z,
    part_up,
    part_y,
    mods,
    halo,
    pre,
    hid,
    c_full,
    snd_c,
    rcv_c,
    snd_l,
    rcv_l,
    snd_t,
    rcv_t,
    snd_b,
    rcv_b,
    snd_o,
    rcv_o,
    weights_like,
    local_sem,
    weight_sem,
    pack_sem,
    line_send,
    line_recv,
    edge_sem,
    flat_send,
    flat_recv,
    o_sem,
):
    s = lax.axis_index("sp")
    t = lax.axis_index("tp")
    d = lax.axis_index("dp")
    z = s // SIDE
    y = lax.rem(s, SIDE)
    own_rows, width = latent.shape
    own_ctx = context.shape[0]
    ctx_rows = SIDE * own_ctx
    depth = mod_weight.shape[1]
    rows = n_tp * own_rows
    inner = w_x.shape[1]
    both = 2 * inner
    head_dim = inner // heads
    nh2 = 2 * heads
    up, down = lax.rem(s + 1, n_sp), lax.rem(s + n_sp - 1, n_sp)

    def remote(src, dst, send, recv, **to):
        return pltpu.make_async_remote_copy(
            src_ref=src, dst_ref=dst, send_sem=send, recv_sem=recv, device_id=to, device_id_type=MESH
        )

    local = []

    def fetch(src, dst):
        copy = pltpu.make_async_copy(src, dst, local_sem.at[len(local)])
        copy.start()
        local.append(copy)
        return copy

    early = [fetch(condition_in, condition), fetch(source_in, source), fetch(mod_weight, mod_buf)]
    barrier = pltpu.get_barrier_semaphore()

    def greet(**to):
        pl.semaphore_signal(barrier, inc=1, device_id=to, device_id_type=MESH)

    def on_z(k):
        return lax.rem(z + k, SIDE) * SIDE + y

    def on_y(k):
        return z * SIDE + lax.rem(y + k, SIDE)

    for k in along():
        greet(sp=on_z(k))
        greet(sp=on_y(k))
    for k in range(1, n_tp):
        greet(tp=lax.rem(t + k, n_tp))
    for k in range(1, n_dp):
        greet(dp=lax.rem(d + k, n_dp))
    z_up, z_down = lax.rem(z + 1, SIDE) * SIDE, lax.rem(z + SIDE - 1, SIDE) * SIDE
    is_first, is_last = s == 0, s == n_sp - 1

    @pl.when(jnp.logical_not(is_first))
    def _():
        greet(sp=down, tp=n_tp - 1)

    @pl.when(jnp.logical_not(is_last))
    def _():
        greet(sp=up, tp=0)


    def settle(ref, sem):
        pltpu.make_async_copy(ref, ref, sem).wait()

    lat_copy = fetch(latent, lat_all.at[t])
    ctx_copy = fetch(context, ctx_buf.at[y])
    small = [
        fetch(a, b)
        for a, b in (
            (gain_in, gain),
            (conv_x_in, conv_x),
            (conv_b_in, conv_b),
            (conv_c_in, conv_c),
            (rate_in, rate),
            (out_gain_in, out_gain),
        )
    ]
    pairs = ((w_x, wx), (w_b, wb), (w_dt, wd), (w_c, wc), (w_z, wz), (w_out, wo))
    places = []
    for src, dst in pairs:
        count = src.shape[0]
        places.append(dst.at[d] if src is w_dt else dst.at[pl.ds(d * count, count)])
        pltpu.make_async_copy(src, places[-1], weight_sem.at[0]).start()

    for copy in early:
        copy.wait()
    acts[0:1] = condition[...].astype(F32)
    acts[1:2] = row_of(source)
    per = LANES // depth
    block = acts[0:2, pl.ds(pl.multiple_of((s // per) * LANES, LANES), LANES)]
    active = jnp.concatenate([silu(block), jnp.zeros((PAD - 2, LANES), F32)], axis=0)
    own_acts = active[:, 0:depth]
    for j in range(1, per):
        own_acts = jnp.where(lax.rem(s, per) == j, active[:, j * depth : (j + 1) * depth], own_acts)
    own_acts = own_acts.astype(BF16)
    pieces = [dot(own_acts, mod_buf[k])[0:2] for k in range(mod_buf.shape[0])]
    cols = pieces[0].shape[1]

    def packed(rows_f32):
        low = [rows_f32[r : r + 1] - rows_f32[r : r + 1].astype(BF16).astype(F32) for r in (0, 2, 4)]
        return jnp.concatenate([rows_f32[0:5]] + low, axis=0).astype(BF16)

    def unpacked(total):
        fine = [total[r : r + 1] + total[5 + r // 2 : 6 + r // 2] for r in (0, 2, 4)]
        return jnp.concatenate(
            [fine[0], total[1:2], fine[1], total[3:4], fine[2], jnp.zeros((3, cols), F32)], axis=0
        )

    partial = jnp.concatenate(pieces + [jnp.zeros((2, cols), F32)], axis=0)
    part[...] = packed(partial)

    lat_copy.wait()
    edges[0] = lat_all[t, 0:1].astype(F32)
    edges[1] = lat_all[t, own_rows - 1 : own_rows].astype(F32)
    ctx_copy.wait()
    edges[2] = ctx_buf[y, 0:1].astype(F32)
    edges[3] = ctx_buf[y, own_ctx - 1 : own_ctx].astype(F32)

    expected = 2 * (SIDE - 1) + n_tp - 1 + n_dp - 1
    sends_up = (t == n_tp - 1) & jnp.logical_not(is_last)
    sends_down = (t == 0) & jnp.logical_not(is_first)
    ctx_sends_up = (y == SIDE - 1) & (z < SIDE - 1)
    ctx_sends_down = (y == 0) & (z > 0)
    expected = expected + jnp.where(sends_up, n_tp, 0) + jnp.where(sends_down, n_tp, 0)
    pl.semaphore_wait(barrier, expected)

    def line(src, dst, place, phase):
        for k in along():
            remote(src, dst.at[k - 1], line_send.at[phase], line_recv.at[phase], sp=place(k)).start()

    def line_wait(dst, phase):
        pltpu.make_async_copy(dst, dst, line_recv.at[phase]).wait()

    line(part, part_z, on_z, 0)
    for k in along():
        remote(ctx_buf.at[y], ctx_buf.at[y], pack_sem.at[2], pack_sem.at[3], sp=on_y(k)).start()
    for k in range(1, n_tp):
        remote(latent, lat_all.at[t], pack_sem.at[0], pack_sem.at[1], tp=lax.rem(t + k, n_tp)).start()
    ctx_up = [
        remote(edges.at[3], halo.at[2], edge_sem.at[0], edge_sem.at[6], sp=z_up + j) for j in range(SIDE)
    ]
    ctx_down = [
        remote(edges.at[2], halo.at[3], edge_sem.at[1], edge_sem.at[7], sp=z_down + j)
        for j in range(SIDE)
    ]
    lat_up = [
        remote(edges.at[1], halo.at[0], edge_sem.at[2], edge_sem.at[4], sp=up, tp=u)
        for u in range(n_tp)
    ]
    lat_down = [
        remote(edges.at[0], halo.at[1], edge_sem.at[3], edge_sem.at[5], sp=down, tp=u)
        for u in range(n_tp)
    ]

    @pl.when(sends_up)
    def _():
        for copy in lat_up:
            copy.start()

    @pl.when(sends_down)
    def _():
        for copy in lat_down:
            copy.start()

    for i, (src, dst) in enumerate(pairs):
        remote(src, places[i], weight_sem.at[1], weight_sem.at[2], dp=1 - d).start()

    def normed(v):
        return v * lax.rsqrt(jnp.mean(v * v, axis=1, keepdims=True) + EPSILON)

    line_wait(part_z, 0)
    others = part_z[0].astype(F32)
    for k in range(2, SIDE):
        others = others + part_z[k - 1].astype(F32)
    summed = partial + unpacked(others)
    part_up[...] = packed(summed)
    line(part_up, part_y, on_y, 1)

    @pl.when(ctx_sends_up)
    def _():
        for copy in ctx_up:
            copy.start()

    @pl.when(ctx_sends_down)
    def _():
        for copy in ctx_down:
            copy.start()


    line_wait(part_y, 1)
    others = part_y[0].astype(F32)
    for k in range(2, SIDE):
        others = others + part_y[k - 1].astype(F32)
    mods[t] = summed + unpacked(others)
    for k in range(1, n_tp):
        remote(mods.at[t], mods.at[t], pack_sem.at[4], pack_sem.at[5], tp=lax.rem(t + k, n_tp)).start()
    settle(lat_all.at[pl.ds(0, n_tp - 1)], pack_sem.at[1])
    for u in range(n_tp):
        pre[u * own_rows : (u + 1) * own_rows] = normed(lat_all[u].astype(F32))
    settle(ctx_buf.at[pl.ds(0, SIDE - 1)], pack_sem.at[3])
    for j in range(0, SIDE, 2):
        pre[rows + PAD + j * own_ctx : rows + PAD + (j + 2) * own_ctx] = normed(
            ctx_buf[j : j + 2].astype(F32).reshape(2 * own_ctx, width)
        )
    inner_edges = (jnp.logical_not(is_first), jnp.logical_not(is_last), z > 0, z < SIDE - 1)
    for j, inside_edge in enumerate(inner_edges):

        @pl.when(inside_edge)
        def _():
            settle(halo.at[j], edge_sem.at[4 + j])

        @pl.when(jnp.logical_not(inside_edge))
        def _():
            halo[j] = jnp.zeros((1, width), F32)

    pre[rows : rows + PAD] = normed(
        jnp.concatenate([halo[0], halo[1], halo[2], halo[3], jnp.zeros((PAD - 4, width), F32)], axis=0)
    )

    for copy in small:
        copy.wait()
    settle(mods.at[pl.ds(0, n_tp - 1)], pack_sem.at[5])

    def vector(row):
        return jnp.concatenate([mods[c][row : row + 1] for c in range(n_tp)], axis=1)

    gain_row = row_of(gain)
    lat_shift, ctx_shift = vector(0), vector(1)
    lat_gain = gain_row * (1.0 + vector(2))
    ctx_gain = gain_row * (1.0 + vector(3))
    for u in range(n_tp):
        cut = slice(u * own_rows, (u + 1) * own_rows)
        hid[cut] = (pre[cut] * lat_gain + lat_shift).astype(BF16)
    at_row = lax.broadcasted_iota(jnp.int32, (PAD, width), 0)
    edge = pre[rows : rows + PAD]
    hid[rows : rows + PAD] = jnp.where(
        at_row < 2, edge * lat_gain + lat_shift, edge * ctx_gain + ctx_shift
    ).astype(BF16)
    hid[rows + PAD : rows + PAD + ctx_rows] = (
        pre[rows + PAD : rows + PAD + ctx_rows] * ctx_gain + ctx_shift
    ).astype(BF16)
    settle(weights_like, weight_sem.at[0])
    settle(weights_like, weight_sem.at[2])

    def shaped(values, before, after, taps, has_before=s > 0, has_after=s < n_sp - 1):
        count = values.shape[0]
        at = lax.broadcasted_iota(jnp.int32, values.shape, 0)
        before = jnp.where(has_before, before, 0.0)
        after = jnp.where(has_after, after, 0.0)
        earlier = jnp.where(at == 0, before, pltpu.roll(values, 1, 0))
        later = jnp.where(at == count - 1, after, pltpu.roll(values, count - 1, 0))
        w = taps[...].astype(F32)
        return silu(earlier * w[0:1] + values * w[1:2] + later * w[2:3]).astype(BF16)

    def project(weight, count):
        return dot(hid[0:count], weight[...]).astype(BF16).astype(F32)

    total = rows + PAD + ctx_rows
    spread_at = lax.broadcasted_iota(jnp.int32, (LANES, both), 0)
    spread_to = lax.broadcasted_iota(jnp.int32, (LANES, both), 1) // head_dim
    spreader = jnp.where((spread_to == spread_at) | (spread_to + nh2 == spread_at), 1.0, 0.0).astype(BF16)

    def expand(v):
        lane = lax.broadcasted_iota(jnp.int32, v.shape, 1)
        high = v.astype(BF16).astype(F32)
        low = pltpu.roll(v - high, nh2, 1)
        packed = jnp.where(lane < nh2, high, jnp.where(lane < 2 * nh2, low, 0.0))
        return dot(packed.astype(BF16), spreader)

    def running(steps):
        count = steps.shape[0]
        logs = -rates * steps
        high = logs.astype(BF16).astype(F32)
        rest = logs - high
        middle = rest.astype(BF16).astype(F32)
        low = rest - middle
        packed = high + pltpu.roll(middle, nh2, 1) + pltpu.roll(low, 2 * nh2, 1)
        a = lax.broadcasted_iota(jnp.int32, (2 * count, count), 0)
        b = lax.broadcasted_iota(jnp.int32, (2 * count, count), 1)
        keep = jnp.where(a < count, jnp.where(a >= b, 1.0, 0.0), jnp.where(a - count <= b, 1.0, 0.0))
        parts = dot(keep.astype(BF16), packed.astype(BF16))
        lane = lax.broadcasted_iota(jnp.int32, (count, LANES), 1)
        parts = jnp.where(lax.rem(lane, nh2) < heads, parts[0:count], parts[count:])
        sums = parts + pltpu.roll(parts, LANES - nh2, 1) + pltpu.roll(parts, LANES - 2 * nh2, 1)
        sums = jnp.where(lane < nh2, sums, 0.0)
        row_lane = lax.broadcasted_iota(jnp.int32, (1, LANES), 1)
        ends = jnp.where(row_lane < heads, sums[count - 1 : count], sums[0:1])
        return sums, ends

    def moved(values, steps):
        wide = jnp.concatenate([values, values], axis=1)
        return (wide * expand(steps)).astype(BF16)

    def spread_out(src, dst, phase):
        for a, b in far_first():
            to = lax.rem(z + a, SIDE) * SIDE + lax.rem(y + b, SIDE)
            remote(src.at[to], dst.at[s], flat_send.at[phase], flat_recv.at[phase], sp=to).start()
        dst[s] = src[s]

    def all_in(dst, phase):
        most = dst.at[pl.ds(0, n_sp - 1)]
        pltpu.make_async_copy(most, most, flat_recv.at[phase]).wait()

    def tiles(dst, state):
        for a in range(SIDE):
            for b in range(SIDE):
                dst[a * SIDE + b] = state[
                    b * TILE : (b + 1) * TILE, a * LANES : (a + 1) * LANES
                ].astype(BF16)

    features = None
    half = wd.shape[3]
    for r in range(n_dp):
        taps = jnp.concatenate(
            [wd[r, 0].astype(F32), wd[r, 1].astype(F32), jnp.zeros((LANES - nh2, half), F32)], axis=0
        ).astype(BF16)
        one = dot(hid[0:total, r * half : (r + 1) * half], taps, ((1,), (1,)))
        features = one if features is None else features + one
    step_all = softplus(features.astype(BF16).astype(F32))
    rates = jnp.concatenate([rate[0:1], rate[1:2], jnp.zeros((1, LANES - nh2), F32)], axis=1)
    c_steps = step_all[rows + PAD :]
    c_sums, c_ends = running(c_steps)
    l_steps = step_all[0:rows]
    l_sums, l_ends = running(l_steps)
    ends = expand(jnp.exp(jnp.concatenate([c_ends, l_ends, jnp.zeros((6, LANES), F32)], axis=0)))
    for a in range(SIDE):
        lanes = ends[1:2, a * LANES : (a + 1) * LANES]
        for b in range(SIDE):
            snd_t[a * SIDE + b] = lanes
    px = project(wx, total)
    pb = project(wb, total)
    x_in = shaped(px[0:rows], px[rows : rows + 1], px[rows + 1 : rows + 2], conv_x).astype(F32)
    b_in = shaped(pb[0:rows], pb[rows : rows + 1], pb[rows + 1 : rows + 2], conv_b)
    l_moved = moved(x_in, l_steps)
    l_scaled = (l_moved.astype(F32) * expand(jnp.exp(l_ends - l_sums))).astype(BF16)
    tiles(snd_l, dot(b_in, l_scaled, ((0,), (0,))))
    spread_out(snd_l, rcv_l, 1)
    spread_out(snd_t, rcv_t, 0)

    c_edges = (z > 0, z < SIDE - 1)
    cx_in = shaped(
        px[rows + PAD :], px[rows + 2 : rows + 3], px[rows + 3 : rows + 4], conv_x, *c_edges
    ).astype(F32)
    cb_in = shaped(pb[rows + PAD :], pb[rows + 2 : rows + 3], pb[rows + 3 : rows + 4], conv_b, *c_edges)
    c_moved = moved(cx_in, c_steps)
    c_scaled = (c_moved.astype(F32) * expand(jnp.exp(c_ends - c_sums))).astype(BF16)
    c_full[...] = dot(cb_in, c_scaled, ((0,), (0,)))
    c_rows = c_full[pl.ds(pl.multiple_of(y * TILE, TILE), TILE)]
    for a in range(SIDE):
        cut = slice(a * LANES, (a + 1) * LANES)
        snd_c[a, 0:TILE] = c_rows[:, cut]
        snd_c[a, TILE : TILE + 8] = jnp.broadcast_to(ends[0:1, cut], (8, LANES))
    for k in along():
        to = lax.rem(z + k, SIDE)
        remote(snd_c.at[to], rcv_c.at[z], line_send.at[2], line_recv.at[2], sp=on_z(k)).start()
    rcv_c[z] = snd_c[z]

    pc = project(wc, rows + PAD)
    c_in = shaped(pc[0:rows], pc[rows : rows + 1], pc[rows + 1 : rows + 2], conv_c)
    scores = dot(c_in, b_in, ((1,), (1,)))
    at_t = lax.broadcasted_iota(jnp.int32, (rows, rows), 0)
    at_s = lax.broadcasted_iota(jnp.int32, (rows, rows), 1)
    sums_t = jnp.transpose(l_sums)

    def weights(lane, keep):
        gap = l_sums[:, lane : lane + 1] - sums_t[lane : lane + 1]
        return jnp.where(keep, scores * jnp.exp(jnp.minimum(gap, 0.0)), 0.0).astype(BF16)

    pair = LANES // head_dim
    inside = []
    lane_head = lax.broadcasted_iota(jnp.int32, (rows, LANES), 1) // head_dim
    for p in range(heads // pair):
        cut = slice(p * LANES, (p + 1) * LANES)
        cut_b = slice(inner + p * LANES, inner + (p + 1) * LANES)
        sources = jnp.concatenate([l_moved[:, cut], l_moved[:, cut_b]], axis=0)
        value = None
        for i in range(pair):
            h = p * pair + i
            w = jnp.concatenate([weights(h, at_t >= at_s), weights(heads + h, at_t <= at_s)], axis=1)
            one = dot(w, sources)
            value = one if value is None else jnp.where(lane_head == i, one, value)
        inside.append(value)
    inside = jnp.concatenate(inside, axis=1)
    growth = expand(jnp.exp(l_sums))
    gate = silu(project(wz, rows))

    forward = z < SIDE // 2

    def place(j, count=n_sp):
        return jnp.where(forward, j, count - 1 - j)

    line_wait(rcv_c.at[pl.ds(0, SIDE - 1)], 2)
    state = jnp.zeros((TILE, LANES), F32)
    for j in range(SIDE):
        i = place(j, SIDE)
        state = state * rcv_c[i, TILE : TILE + 1] + rcv_c[i, 0:TILE]
    all_in(rcv_t, 0)
    all_in(rcv_l, 1)

    def latent_step(j, state):
        i = place(j)
        snd_b[i] = state.astype(BF16)
        return state * rcv_t[i] + rcv_l[i].astype(F32)

    lax.fori_loop(0, n_sp, latent_step, state, unroll=8)
    for row in range(SIDE):
        for b in along():
            to = row * SIDE + lax.rem(y + b, SIDE)
            remote(snd_b.at[to], rcv_b.at[s], flat_send.at[2], flat_recv.at[2], sp=to).start()

        @pl.when(z != row)
        def _():
            to = row * SIDE + y
            remote(snd_b.at[to], rcv_b.at[s], flat_send.at[2], flat_recv.at[2], sp=to).start()

    rcv_b[s] = snd_b[s]
    all_in(rcv_b, 2)
    entering = jnp.concatenate(
        [rcv_b[a * SIDE : (a + 1) * SIDE].reshape(STATE, LANES) for a in range(SIDE)], axis=1
    )
    carried = dot(c_in, entering) * growth
    gated = (inside + carried[:, 0:inner] + carried[:, inner:both]) * gate
    ny = (
        gated
        * lax.rsqrt(jnp.mean(gated * gated, axis=1, keepdims=True) + EPSILON)
        * row_of(out_gain)
    ).astype(BF16)

    chunks = n_tp
    chunk = width // chunks
    far_tp = sorted(range(1, n_tp), key=lambda k: -min(k, n_tp - k))
    for c in range(chunks):
        cut = slice(c * chunk, (c + 1) * chunk)
        result = dot(ny, wo[:, cut]).astype(BF16)
        for u in range(n_tp):
            snd_o[c, u] = result[u * own_rows : (u + 1) * own_rows]
        for k in far_tp:
            to = lax.rem(t + k, n_tp)
            remote(snd_o.at[c, to], rcv_o.at[c, k - 1], o_sem.at[chunks], o_sem.at[c], tp=to).start()

    for phase, sent in ((0, part_z), (1, part_y), (2, rcv_c.at[pl.ds(0, SIDE - 1)])):
        settle(sent, line_send.at[phase])
    for phase, sent in ((0, rcv_t), (1, rcv_l), (2, rcv_b)):
        settle(sent.at[pl.ds(0, n_sp - 1)], flat_send.at[phase])
    settle(weights_like, weight_sem.at[1])
    settle(lat_all.at[pl.ds(0, n_tp - 1)], pack_sem.at[0])
    settle(ctx_buf.at[pl.ds(0, SIDE - 1)], pack_sem.at[2])
    settle(mods.at[pl.ds(0, n_tp - 1)], pack_sem.at[4])

    for j, (ref, sends) in enumerate(
        ((acts, ctx_sends_up), (acts, ctx_sends_down), (halo, sends_up), (halo, sends_down))
    ):

        @pl.when(sends)
        def _():
            settle(ref, edge_sem.at[j])


    for c in range(chunks):
        mixed = snd_o[c, t].astype(F32)
        settle(rcv_o.at[c], o_sem.at[c])
        for k in range(1, n_tp):
            mixed = mixed + rcv_o[c, k - 1].astype(F32)
        out[:, c * chunk : (c + 1) * chunk] = (mods[c][4:5] * mixed).astype(BF16)
    settle(rcv_o, o_sem.at[chunks])


def shards(
    latent,
    condition,
    context,
    context_source,
    mod_weight,
    norm_gain,
    w_x,
    w_b,
    w_c,
    w_z,
    w_dt,
    conv_x,
    conv_b,
    conv_c,
    decay_rate,
    out_gain,
    w_out,
):
    n_sp, n_tp, n_dp = lax.axis_size("sp"), lax.axis_size("tp"), lax.axis_size("dp")
    assert n_sp == SIDE * SIDE
    own_rows, width = latent.shape[1:]
    own_ctx = context.shape[1]
    ctx_rows = SIDE * own_ctx
    cols = mod_weight.shape[2]
    inner = w_x.shape[1]
    heads = decay_rate.shape[1]
    assert STATE == SIDE * TILE and 2 * inner == SIDE * LANES
    rows = n_tp * own_rows
    total = rows + PAD + ctx_rows
    chunk = width // n_tp
    vmem = pl.BlockSpec(memory_space=pltpu.VMEM)
    anywhere = pl.BlockSpec(memory_space=pl.ANY)
    dma = pltpu.SemaphoreType.DMA
    args = (
        condition,
        context_source,
        norm_gain,
        conv_x,
        conv_b,
        conv_c,
        decay_rate,
        out_gain,
        latent[0],
        context[0],
        mod_weight,
        w_x,
        w_b,
        w_c,
        jnp.swapaxes(w_dt, 1, 2),
        w_z,
        w_out,
    )
    tiles = pltpu.VMEM((n_sp, TILE, LANES), BF16)
    sent_rows = sum(w.size for w in (w_x, w_b, w_c, w_dt, w_z, w_out)) // width
    scratch = [pltpu.VMEM(a.shape, a.dtype) for a in args[:8]] + [
        pltpu.VMEM((n_tp, own_rows, width), BF16),
        pltpu.VMEM((SIDE, own_ctx, width), BF16),
        pltpu.VMEM(mod_weight.shape, BF16),
        pltpu.VMEM((w_x.shape[0] * n_dp, inner), BF16),
        pltpu.VMEM((w_b.shape[0] * n_dp, w_b.shape[1]), BF16),
        pltpu.VMEM((w_c.shape[0] * n_dp, w_c.shape[1]), BF16),
        pltpu.VMEM((n_dp, 2, heads, w_dt.shape[1]), BF16),
        pltpu.VMEM((w_z.shape[0] * n_dp, inner), BF16),
        pltpu.VMEM((w_out.shape[0] * n_dp, width), BF16),
        pltpu.VMEM((8, width), F32),
        pltpu.VMEM((4, 1, width), F32),
        pltpu.VMEM((8, cols), BF16),
        pltpu.VMEM((SIDE - 1, 8, cols), BF16),
        pltpu.VMEM((8, cols), BF16),
        pltpu.VMEM((SIDE - 1, 8, cols), BF16),
        pltpu.VMEM((n_tp, 8, cols), F32),
        pltpu.VMEM((4, 1, width), F32),
        pltpu.VMEM((total, width), F32),
        pltpu.VMEM((total, width), BF16),
        pltpu.VMEM((STATE, 2 * inner), F32),
        pltpu.VMEM((SIDE, TILE + 8, LANES), F32),
        pltpu.VMEM((SIDE, TILE + 8, LANES), F32),
        tiles,
        tiles,
        pltpu.VMEM((n_sp, 1, LANES), F32),
        pltpu.VMEM((n_sp, 1, LANES), F32),
        tiles,
        tiles,
        pltpu.VMEM((n_tp, n_tp, own_rows, chunk), BF16),
        pltpu.VMEM((n_tp, n_tp - 1, own_rows, chunk), BF16),
        pltpu.VMEM((sent_rows, width), BF16),
        dma((11,)),
        dma((3,)),
        dma((6,)),
        dma((3,)),
        dma((3,)),
        dma((8,)),
        dma((3,)),
        dma((3,)),
        dma((n_tp + 1,)),
    ]
    result = pl.pallas_call(
        functools.partial(kernel, n_sp, n_tp, n_dp, heads),
        out_shape=pltpu.VMEM((own_rows, width), BF16),
        in_specs=[anywhere] * len(args),
        out_specs=vmem,
        scratch_shapes=scratch,
        compiler_params=pltpu.CompilerParams(
            collective_id=0, has_side_effects=True, vmem_limit_bytes=62_000_000
        ),
    )(*args)
    return result[None]


def solution(mesh):
    placed = (
        P("dp", ("sp", "tp"), None),
        P("dp", None),
        P("dp", "sp", None),
        P(),
        P(None, "sp", "tp"),
        P(),
        P("dp", "tp"),
        P("dp", "tp"),
        P("dp", "tp"),
        P("dp", "tp"),
        P(None, "dp", "tp"),
        P(None, "tp"),
        P(None, "tp"),
        P(None, "tp"),
        P(None, "tp"),
        P("tp"),
        P(("tp", "dp"), None),
    )
    return jax.shard_map(
        shards, mesh=mesh, in_specs=placed, out_specs=P("dp", ("sp", "tp"), None), check_vma=False
    )
```

```python
import functools

import jax
import jax.numpy as jnp
from jax import lax
from jax.experimental import pallas as pl
from jax.experimental.pallas import tpu as pltpu
from jax.sharding import PartitionSpec as P

STATE = 128
LANES = 128
PAD = 16
SIDE = 8
TILE = 16
EPSILON = 1e-06
MESH = pl.DeviceIdType.MESH
F32 = jnp.float32
BF16 = jnp.bfloat16


def silu(v):
    return v / (1.0 + jnp.exp(-v))


def softplus(v):
    return jnp.maximum(v, 0.0) + jnp.log1p(jnp.exp(-jnp.abs(v)))


def row_of(ref):
    return ref[...].astype(F32).reshape(1, ref.shape[0])


def dot(a, b, dims=((1,), (0,)), precision=None):
    return lax.dot_general(a, b, (dims, ((), ())), precision=precision, preferred_element_type=F32)


def reach(k):
    return min(k, SIDE - k)


def along():
    return sorted(range(1, SIDE), key=lambda k: -reach(k))


def far_first():
    steps = [(a, b) for a in range(SIDE) for b in range(SIDE) if a or b]
    return sorted(steps, key=lambda ab: -(reach(ab[0]) + reach(ab[1])))


def kernel(
    n_sp,
    n_tp,
    n_dp,
    heads,
    condition_in,
    source_in,
    gain_in,
    conv_x_in,
    conv_b_in,
    conv_c_in,
    rate_in,
    out_gain_in,
    latent,
    context,
    mod_weight,
    w_x,
    w_b,
    w_c,
    w_dt,
    w_z,
    w_out,
    out,
    condition,
    source,
    gain,
    conv_x,
    conv_b,
    conv_c,
    rate,
    out_gain,
    lat_all,
    ctx_buf,
    mod_buf,
    wx,
    wb,
    wc,
    wd,
    wz,
    wo,
    acts,
    edges,
    part,
    part_z,
    part_up,
    part_y,
    mods,
    halo,
    pre,
    hid,
    c_full,
    snd_c,
    rcv_c,
    snd_l,
    rcv_l,
    snd_t,
    rcv_t,
    snd_b,
    rcv_b,
    snd_o,
    rcv_o,
    weights_like,
    local_sem,
    weight_sem,
    pack_sem,
    line_send,
    line_recv,
    edge_sem,
    flat_send,
    flat_recv,
    o_sem,
):
    s = lax.axis_index("sp")
    t = lax.axis_index("tp")
    d = lax.axis_index("dp")
    z = s // SIDE
    y = lax.rem(s, SIDE)
    own_rows, width = latent.shape
    own_ctx = context.shape[0]
    ctx_rows = SIDE * own_ctx
    depth = mod_weight.shape[1]
    rows = n_tp * own_rows
    inner = w_x.shape[1]
    both = 2 * inner
    head_dim = inner // heads
    nh2 = 2 * heads
    up, down = lax.rem(s + 1, n_sp), lax.rem(s + n_sp - 1, n_sp)

    def remote(src, dst, send, recv, **to):
        return pltpu.make_async_remote_copy(
            src_ref=src, dst_ref=dst, send_sem=send, recv_sem=recv, device_id=to, device_id_type=MESH
        )

    local = []

    def fetch(src, dst):
        copy = pltpu.make_async_copy(src, dst, local_sem.at[len(local)])
        copy.start()
        local.append(copy)
        return copy

    early = [fetch(condition_in, condition), fetch(source_in, source), fetch(mod_weight, mod_buf)]
    barrier = pltpu.get_barrier_semaphore()

    def greet(**to):
        pl.semaphore_signal(barrier, inc=1, device_id=to, device_id_type=MESH)

    def on_z(k):
        return lax.rem(z + k, SIDE) * SIDE + y

    def on_y(k):
        return z * SIDE + lax.rem(y + k, SIDE)

    for k in along():
        greet(sp=on_z(k))
        greet(sp=on_y(k))
    for k in range(1, n_tp):
        greet(tp=lax.rem(t + k, n_tp))
    for k in range(1, n_dp):
        greet(dp=lax.rem(d + k, n_dp))
    z_up, z_down = lax.rem(z + 1, SIDE) * SIDE, lax.rem(z + SIDE - 1, SIDE) * SIDE
    is_first, is_last = s == 0, s == n_sp - 1

    @pl.when(jnp.logical_not(is_first))
    def _():
        greet(sp=down, tp=n_tp - 1)

    @pl.when(jnp.logical_not(is_last))
    def _():
        greet(sp=up, tp=0)


    def settle(ref, sem):
        pltpu.make_async_copy(ref, ref, sem).wait()

    lat_copy = fetch(latent, lat_all.at[t])
    ctx_copy = fetch(context, ctx_buf.at[y])
    small = [
        fetch(a, b)
        for a, b in (
            (gain_in, gain),
            (conv_x_in, conv_x),
            (conv_b_in, conv_b),
            (conv_c_in, conv_c),
            (rate_in, rate),
            (out_gain_in, out_gain),
        )
    ]
    pairs = ((w_x, wx), (w_b, wb), (w_dt, wd), (w_c, wc), (w_z, wz), (w_out, wo))
    places = []
    for src, dst in pairs:
        count = src.shape[0]
        places.append(dst.at[d] if src is w_dt else dst.at[pl.ds(d * count, count)])
        pltpu.make_async_copy(src, places[-1], weight_sem.at[0]).start()

    for copy in early:
        copy.wait()
    acts[0:1] = condition[...].astype(F32)
    acts[1:2] = row_of(source)
    per = LANES // depth
    block = acts[0:2, pl.ds(pl.multiple_of((s // per) * LANES, LANES), LANES)]
    active = jnp.concatenate([silu(block), jnp.zeros((PAD - 2, LANES), F32)], axis=0)
    own_acts = active[:, 0:depth]
    for j in range(1, per):
        own_acts = jnp.where(lax.rem(s, per) == j, active[:, j * depth : (j + 1) * depth], own_acts)
    own_acts = own_acts.astype(BF16)
    pieces = [dot(own_acts, mod_buf[k])[0:2] for k in range(mod_buf.shape[0])]
    cols = pieces[0].shape[1]

    def packed(rows_f32):
        low = [rows_f32[r : r + 1] - rows_f32[r : r + 1].astype(BF16).astype(F32) for r in (0, 2, 4)]
        return jnp.concatenate([rows_f32[0:5]] + low, axis=0).astype(BF16)

    def unpacked(total):
        fine = [total[r : r + 1] + total[5 + r // 2 : 6 + r // 2] for r in (0, 2, 4)]
        return jnp.concatenate(
            [fine[0], total[1:2], fine[1], total[3:4], fine[2], jnp.zeros((3, cols), F32)], axis=0
        )

    partial = jnp.concatenate(pieces + [jnp.zeros((2, cols), F32)], axis=0)
    part[...] = packed(partial)

    lat_copy.wait()
    edges[0] = lat_all[t, 0:1].astype(F32)
    edges[1] = lat_all[t, own_rows - 1 : own_rows].astype(F32)
    ctx_copy.wait()
    edges[2] = ctx_buf[y, 0:1].astype(F32)
    edges[3] = ctx_buf[y, own_ctx - 1 : own_ctx].astype(F32)

    expected = 2 * (SIDE - 1) + n_tp - 1 + n_dp - 1
    sends_up = (t == n_tp - 1) & jnp.logical_not(is_last)
    sends_down = (t == 0) & jnp.logical_not(is_first)
    ctx_sends_up = (y == SIDE - 1) & (z < SIDE - 1)
    ctx_sends_down = (y == 0) & (z > 0)
    expected = expected + jnp.where(sends_up, n_tp, 0) + jnp.where(sends_down, n_tp, 0)
    pl.semaphore_wait(barrier, expected)

    def line(src, dst, place, phase):
        for k in along():
            remote(src, dst.at[k - 1], line_send.at[phase], line_recv.at[phase], sp=place(k)).start()

    def line_wait(dst, phase):
        pltpu.make_async_copy(dst, dst, line_recv.at[phase]).wait()

    line(part, part_z, on_z, 0)
    for k in along():
        remote(ctx_buf.at[y], ctx_buf.at[y], pack_sem.at[2], pack_sem.at[3], sp=on_y(k)).start()
    for k in range(1, n_tp):
        remote(latent, lat_all.at[t], pack_sem.at[0], pack_sem.at[1], tp=lax.rem(t + k, n_tp)).start()
    ctx_up = [
        remote(edges.at[3], halo.at[2], edge_sem.at[0], edge_sem.at[6], sp=z_up + j) for j in range(SIDE)
    ]
    ctx_down = [
        remote(edges.at[2], halo.at[3], edge_sem.at[1], edge_sem.at[7], sp=z_down + j)
        for j in range(SIDE)
    ]
    lat_up = [
        remote(edges.at[1], halo.at[0], edge_sem.at[2], edge_sem.at[4], sp=up, tp=u)
        for u in range(n_tp)
    ]
    lat_down = [
        remote(edges.at[0], halo.at[1], edge_sem.at[3], edge_sem.at[5], sp=down, tp=u)
        for u in range(n_tp)
    ]

    @pl.when(sends_up)
    def _():
        for copy in lat_up:
            copy.start()

    @pl.when(sends_down)
    def _():
        for copy in lat_down:
            copy.start()

    for i, (src, dst) in enumerate(pairs):
        remote(src, places[i], weight_sem.at[1], weight_sem.at[2], dp=1 - d).start()

    def normed(v):
        return v * lax.rsqrt(jnp.mean(v * v, axis=1, keepdims=True) + EPSILON)

    line_wait(part_z, 0)
    others = part_z[0].astype(F32)
    for k in range(2, SIDE):
        others = others + part_z[k - 1].astype(F32)
    summed = partial + unpacked(others)
    part_up[...] = packed(summed)
    line(part_up, part_y, on_y, 1)

    @pl.when(ctx_sends_up)
    def _():
        for copy in ctx_up:
            copy.start()

    @pl.when(ctx_sends_down)
    def _():
        for copy in ctx_down:
            copy.start()


    line_wait(part_y, 1)
    others = part_y[0].astype(F32)
    for k in range(2, SIDE):
        others = others + part_y[k - 1].astype(F32)
    mods[t] = summed + unpacked(others)
    for k in range(1, n_tp):
        remote(mods.at[t], mods.at[t], pack_sem.at[4], pack_sem.at[5], tp=lax.rem(t + k, n_tp)).start()
    settle(lat_all.at[pl.ds(0, n_tp - 1)], pack_sem.at[1])
    for u in range(n_tp):
        pre[u * own_rows : (u + 1) * own_rows] = normed(lat_all[u].astype(F32))
    settle(ctx_buf.at[pl.ds(0, SIDE - 1)], pack_sem.at[3])
    for j in range(0, SIDE, 2):
        pre[rows + PAD + j * own_ctx : rows + PAD + (j + 2) * own_ctx] = normed(
            ctx_buf[j : j + 2].astype(F32).reshape(2 * own_ctx, width)
        )
    inner_edges = (jnp.logical_not(is_first), jnp.logical_not(is_last), z > 0, z < SIDE - 1)
    for j, inside_edge in enumerate(inner_edges):

        @pl.when(inside_edge)
        def _():
            settle(halo.at[j], edge_sem.at[4 + j])

        @pl.when(jnp.logical_not(inside_edge))
        def _():
            halo[j] = jnp.zeros((1, width), F32)

    pre[rows : rows + PAD] = normed(
        jnp.concatenate([halo[0], halo[1], halo[2], halo[3], jnp.zeros((PAD - 4, width), F32)], axis=0)
    )

    for copy in small:
        copy.wait()
    settle(mods.at[pl.ds(0, n_tp - 1)], pack_sem.at[5])

    def vector(row):
        return jnp.concatenate([mods[c][row : row + 1] for c in range(n_tp)], axis=1)

    gain_row = row_of(gain)
    lat_shift, ctx_shift = vector(0), vector(1)
    lat_gain = gain_row * (1.0 + vector(2))
    ctx_gain = gain_row * (1.0 + vector(3))
    for u in range(n_tp):
        cut = slice(u * own_rows, (u + 1) * own_rows)
        hid[cut] = (pre[cut] * lat_gain + lat_shift).astype(BF16)
    at_row = lax.broadcasted_iota(jnp.int32, (PAD, width), 0)
    edge = pre[rows : rows + PAD]
    hid[rows : rows + PAD] = jnp.where(
        at_row < 2, edge * lat_gain + lat_shift, edge * ctx_gain + ctx_shift
    ).astype(BF16)
    settle(weights_like, weight_sem.at[0])
    settle(weights_like, weight_sem.at[2])

    def shaped(values, before, after, taps, has_before=s > 0, has_after=s < n_sp - 1):
        count = values.shape[0]
        at = lax.broadcasted_iota(jnp.int32, values.shape, 0)
        before = jnp.where(has_before, before, 0.0)
        after = jnp.where(has_after, after, 0.0)
        earlier = jnp.where(at == 0, before, pltpu.roll(values, 1, 0))
        later = jnp.where(at == count - 1, after, pltpu.roll(values, count - 1, 0))
        w = taps[...].astype(F32)
        return silu(earlier * w[0:1] + values * w[1:2] + later * w[2:3]).astype(BF16)

    def project(weight, first, last):
        return dot(hid[first:last], weight[...]).astype(BF16).astype(F32)

    total = rows + PAD + ctx_rows
    half = wd.shape[3]
    spread_at = lax.broadcasted_iota(jnp.int32, (LANES, both), 0)
    spread_to = lax.broadcasted_iota(jnp.int32, (LANES, both), 1) // head_dim
    spreader = jnp.where((spread_to == spread_at) | (spread_to + nh2 == spread_at), 1.0, 0.0).astype(BF16)

    def expand(v):
        lane = lax.broadcasted_iota(jnp.int32, v.shape, 1)
        high = v.astype(BF16).astype(F32)
        low = pltpu.roll(v - high, nh2, 1)
        packed = jnp.where(lane < nh2, high, jnp.where(lane < 2 * nh2, low, 0.0))
        return dot(packed.astype(BF16), spreader)

    def running(steps):
        count = steps.shape[0]
        logs = -rates * steps
        high = logs.astype(BF16).astype(F32)
        rest = logs - high
        middle = rest.astype(BF16).astype(F32)
        low = rest - middle
        packed = high + pltpu.roll(middle, nh2, 1) + pltpu.roll(low, 2 * nh2, 1)
        a = lax.broadcasted_iota(jnp.int32, (2 * count, count), 0)
        b = lax.broadcasted_iota(jnp.int32, (2 * count, count), 1)
        keep = jnp.where(a < count, jnp.where(a >= b, 1.0, 0.0), jnp.where(a - count <= b, 1.0, 0.0))
        parts = dot(keep.astype(BF16), packed.astype(BF16))
        lane = lax.broadcasted_iota(jnp.int32, (count, LANES), 1)
        parts = jnp.where(lax.rem(lane, nh2) < heads, parts[0:count], parts[count:])
        sums = parts + pltpu.roll(parts, LANES - nh2, 1) + pltpu.roll(parts, LANES - 2 * nh2, 1)
        sums = jnp.where(lane < nh2, sums, 0.0)
        row_lane = lax.broadcasted_iota(jnp.int32, (1, LANES), 1)
        ends = jnp.where(row_lane < heads, sums[count - 1 : count], sums[0:1])
        return sums, ends

    def moved(values, steps):
        wide = jnp.concatenate([values, values], axis=1)
        return (wide * expand(steps)).astype(BF16)

    def spread_out(src, dst, phase):
        for a, b in far_first():
            to = lax.rem(z + a, SIDE) * SIDE + lax.rem(y + b, SIDE)
            remote(src.at[to], dst.at[s], flat_send.at[phase], flat_recv.at[phase], sp=to).start()
        dst[s] = src[s]

    def all_in(dst, phase):
        most = dst.at[pl.ds(0, n_sp - 1)]
        pltpu.make_async_copy(most, most, flat_recv.at[phase]).wait()

    def tiles(dst, state):
        for a in range(SIDE):
            for b in range(SIDE):
                dst[a * SIDE + b] = state[
                    b * TILE : (b + 1) * TILE, a * LANES : (a + 1) * LANES
                ].astype(BF16)

    dt_taps = [
        jnp.concatenate(
            [wd[r, 0].astype(F32), wd[r, 1].astype(F32), jnp.zeros((LANES - nh2, half), F32)], axis=0
        ).astype(BF16)
        for r in range(n_dp)
    ]

    def steps_of(first, last):
        features = None
        for r in range(n_dp):
            one = dot(hid[first:last, r * half : (r + 1) * half], dt_taps[r], ((1,), (1,)))
            features = one if features is None else features + one
        return softplus(features.astype(BF16).astype(F32))

    rates = jnp.concatenate([rate[0:1], rate[1:2], jnp.zeros((1, LANES - nh2), F32)], axis=1)
    l_steps = steps_of(0, rows)
    l_sums, l_ends = running(l_steps)
    ends = expand(jnp.exp(jnp.broadcast_to(l_ends, (8, LANES))))
    for a in range(SIDE):
        snd_t[a] = ends[0:1, a * LANES : (a + 1) * LANES]
    px = project(wx, 0, rows + PAD)
    pb = project(wb, 0, rows + PAD)
    x_in = shaped(px[0:rows], px[rows : rows + 1], px[rows + 1 : rows + 2], conv_x).astype(F32)
    b_in = shaped(pb[0:rows], pb[rows : rows + 1], pb[rows + 1 : rows + 2], conv_b)
    l_moved = moved(x_in, l_steps)
    l_scaled = (l_moved.astype(F32) * expand(jnp.exp(l_ends - l_sums))).astype(BF16)
    tiles(snd_l, dot(b_in, l_scaled, ((0,), (0,))))
    spread_out(snd_l, rcv_l, 0)
    for a, b in far_first():
        row = lax.rem(z + a, SIDE)
        to = row * SIDE + lax.rem(y + b, SIDE)
        remote(snd_t.at[row], rcv_t.at[s], flat_send.at[2], flat_recv.at[2], sp=to).start()
    rcv_t[s] = snd_t[z]

    hid[rows + PAD : rows + PAD + ctx_rows] = (
        pre[rows + PAD : rows + PAD + ctx_rows] * ctx_gain + ctx_shift
    ).astype(BF16)
    c_steps = steps_of(rows + PAD, total)
    c_sums, c_ends = running(c_steps)
    c_decay = expand(jnp.exp(jnp.broadcast_to(c_ends, (8, LANES))))
    cpx = project(wx, rows, total)
    cpb = project(wb, rows, total)
    c_edges = (z > 0, z < SIDE - 1)
    cx_in = shaped(cpx[PAD:], cpx[2:3], cpx[3:4], conv_x, *c_edges).astype(F32)
    cb_in = shaped(cpb[PAD:], cpb[2:3], cpb[3:4], conv_b, *c_edges)
    c_moved = moved(cx_in, c_steps)
    c_scaled = (c_moved.astype(F32) * expand(jnp.exp(c_ends - c_sums))).astype(BF16)
    c_full[...] = dot(cb_in, c_scaled, ((0,), (0,)))
    c_rows = c_full[pl.ds(pl.multiple_of(y * TILE, TILE), TILE)]
    c_high = c_decay.astype(BF16).astype(F32)
    c_tail = jnp.where(lax.broadcasted_iota(jnp.int32, c_decay.shape, 0) == 0, c_high, c_decay - c_high)
    c_all = jnp.concatenate([c_rows, c_tail], axis=0).astype(BF16)
    for a in range(SIDE):
        snd_c[a] = c_all[:, a * LANES : (a + 1) * LANES]
    for k in along():
        to = lax.rem(z + k, SIDE)
        remote(snd_c.at[to], rcv_c.at[z], line_send.at[2], line_recv.at[2], sp=on_z(k)).start()
    rcv_c[z] = snd_c[z]

    pc = project(wc, 0, rows + PAD)
    c_in = shaped(pc[0:rows], pc[rows : rows + 1], pc[rows + 1 : rows + 2], conv_c)
    scores = dot(c_in, b_in, ((1,), (1,)))
    at_t = lax.broadcasted_iota(jnp.int32, (rows, rows), 0)
    at_s = lax.broadcasted_iota(jnp.int32, (rows, rows), 1)
    sums_t = jnp.transpose(l_sums)

    def weights(lane, keep):
        gap = l_sums[:, lane : lane + 1] - sums_t[lane : lane + 1]
        return jnp.where(keep, scores * jnp.exp(jnp.minimum(gap, 0.0)), 0.0).astype(BF16)

    pair = LANES // head_dim
    inside = []
    lane_head = lax.broadcasted_iota(jnp.int32, (rows, LANES), 1) // head_dim
    for p in range(heads // pair):
        cut = slice(p * LANES, (p + 1) * LANES)
        cut_b = slice(inner + p * LANES, inner + (p + 1) * LANES)
        sources = jnp.concatenate([l_moved[:, cut], l_moved[:, cut_b]], axis=0)
        value = None
        for i in range(pair):
            h = p * pair + i
            w = jnp.concatenate([weights(h, at_t >= at_s), weights(heads + h, at_t <= at_s)], axis=1)
            one = dot(w, sources)
            value = one if value is None else jnp.where(lane_head == i, one, value)
        inside.append(value)
    inside = jnp.concatenate(inside, axis=1)
    growth = expand(jnp.exp(l_sums))
    gate = silu(project(wz, 0, rows))

    forward = z < SIDE // 2

    def place(j, count=n_sp):
        return jnp.where(forward, j, count - 1 - j)

    line_wait(rcv_c.at[pl.ds(0, SIDE - 1)], 2)
    state = jnp.zeros((TILE, LANES), F32)
    for j in range(SIDE):
        i = place(j, SIDE)
        piece = rcv_c[i].astype(F32)
        state = state * (piece[TILE : TILE + 1] + piece[TILE + 1 : TILE + 2]) + piece[0:TILE]
    all_in(rcv_t, 2)
    all_in(rcv_l, 0)

    def latent_step(j, state):
        i = place(j)
        snd_b[i] = state.astype(BF16)
        return state * rcv_t[i] + rcv_l[i].astype(F32)

    lax.fori_loop(0, n_sp, latent_step, state, unroll=8)
    for row in range(SIDE):
        for b in along():
            to = row * SIDE + lax.rem(y + b, SIDE)
            remote(snd_b.at[to], rcv_b.at[s], flat_send.at[1], flat_recv.at[1], sp=to).start()

        @pl.when(z != row)
        def _():
            to = row * SIDE + y
            remote(snd_b.at[to], rcv_b.at[s], flat_send.at[1], flat_recv.at[1], sp=to).start()

    rcv_b[s] = snd_b[s]
    all_in(rcv_b, 1)
    entering = jnp.concatenate(
        [rcv_b[a * SIDE : (a + 1) * SIDE].reshape(STATE, LANES) for a in range(SIDE)], axis=1
    )
    carried = dot(c_in, entering) * growth
    gated = (inside + carried[:, 0:inner] + carried[:, inner:both]) * gate
    ny = (
        gated
        * lax.rsqrt(jnp.mean(gated * gated, axis=1, keepdims=True) + EPSILON)
        * row_of(out_gain)
    ).astype(BF16)

    chunks = n_tp
    chunk = width // chunks
    far_tp = sorted(range(1, n_tp), key=lambda k: -min(k, n_tp - k))
    for c in range(chunks):
        cut = slice(c * chunk, (c + 1) * chunk)
        result = dot(ny, wo[:, cut]).astype(BF16)
        for u in range(n_tp):
            snd_o[c, u] = result[u * own_rows : (u + 1) * own_rows]
        for k in far_tp:
            to = lax.rem(t + k, n_tp)
            remote(snd_o.at[c, to], rcv_o.at[c, k - 1], o_sem.at[chunks], o_sem.at[c], tp=to).start()

    most = pl.ds(0, SIDE - 1)
    for phase, sent in enumerate((part_z, part_y, rcv_c.at[most])):
        settle(sent, line_send.at[phase])
    for phase, sent in enumerate((rcv_l, rcv_b, rcv_t)):
        settle(sent.at[pl.ds(0, n_sp - 1)], flat_send.at[phase])
    settle(weights_like, weight_sem.at[1])
    settle(lat_all.at[pl.ds(0, n_tp - 1)], pack_sem.at[0])
    settle(ctx_buf.at[pl.ds(0, SIDE - 1)], pack_sem.at[2])
    settle(mods.at[pl.ds(0, n_tp - 1)], pack_sem.at[4])

    for j, (ref, sends) in enumerate(
        ((acts, ctx_sends_up), (acts, ctx_sends_down), (halo, sends_up), (halo, sends_down))
    ):

        @pl.when(sends)
        def _():
            settle(ref, edge_sem.at[j])


    for c in range(chunks):
        mixed = snd_o[c, t].astype(F32)
        settle(rcv_o.at[c], o_sem.at[c])
        for k in range(1, n_tp):
            mixed = mixed + rcv_o[c, k - 1].astype(F32)
        out[:, c * chunk : (c + 1) * chunk] = (mods[c][4:5] * mixed).astype(BF16)
    settle(rcv_o, o_sem.at[chunks])


def shards(
    latent,
    condition,
    context,
    context_source,
    mod_weight,
    norm_gain,
    w_x,
    w_b,
    w_c,
    w_z,
    w_dt,
    conv_x,
    conv_b,
    conv_c,
    decay_rate,
    out_gain,
    w_out,
):
    n_sp, n_tp, n_dp = lax.axis_size("sp"), lax.axis_size("tp"), lax.axis_size("dp")
    assert n_sp == SIDE * SIDE
    own_rows, width = latent.shape[1:]
    own_ctx = context.shape[1]
    ctx_rows = SIDE * own_ctx
    cols = mod_weight.shape[2]
    inner = w_x.shape[1]
    heads = decay_rate.shape[1]
    assert STATE == SIDE * TILE and 2 * inner == SIDE * LANES
    rows = n_tp * own_rows
    total = rows + PAD + ctx_rows
    chunk = width // n_tp
    vmem = pl.BlockSpec(memory_space=pltpu.VMEM)
    anywhere = pl.BlockSpec(memory_space=pl.ANY)
    dma = pltpu.SemaphoreType.DMA
    args = (
        condition,
        context_source,
        norm_gain,
        conv_x,
        conv_b,
        conv_c,
        decay_rate,
        out_gain,
        latent[0],
        context[0],
        mod_weight,
        w_x,
        w_b,
        w_c,
        jnp.swapaxes(w_dt, 1, 2),
        w_z,
        w_out,
    )
    tiles = pltpu.VMEM((n_sp, TILE, LANES), BF16)
    sent_rows = sum(w.size for w in (w_x, w_b, w_c, w_dt, w_z, w_out)) // width
    scratch = [pltpu.VMEM(a.shape, a.dtype) for a in args[:8]] + [
        pltpu.VMEM((n_tp, own_rows, width), BF16),
        pltpu.VMEM((SIDE, own_ctx, width), BF16),
        pltpu.VMEM(mod_weight.shape, BF16),
        pltpu.VMEM((w_x.shape[0] * n_dp, inner), BF16),
        pltpu.VMEM((w_b.shape[0] * n_dp, w_b.shape[1]), BF16),
        pltpu.VMEM((w_c.shape[0] * n_dp, w_c.shape[1]), BF16),
        pltpu.VMEM((n_dp, 2, heads, w_dt.shape[1]), BF16),
        pltpu.VMEM((w_z.shape[0] * n_dp, inner), BF16),
        pltpu.VMEM((w_out.shape[0] * n_dp, width), BF16),
        pltpu.VMEM((8, width), F32),
        pltpu.VMEM((4, 1, width), F32),
        pltpu.VMEM((8, cols), BF16),
        pltpu.VMEM((SIDE - 1, 8, cols), BF16),
        pltpu.VMEM((8, cols), BF16),
        pltpu.VMEM((SIDE - 1, 8, cols), BF16),
        pltpu.VMEM((n_tp, 8, cols), F32),
        pltpu.VMEM((4, 1, width), F32),
        pltpu.VMEM((total, width), F32),
        pltpu.VMEM((total, width), BF16),
        pltpu.VMEM((STATE, 2 * inner), F32),
        pltpu.VMEM((SIDE, TILE + 8, LANES), BF16),
        pltpu.VMEM((SIDE, TILE + 8, LANES), BF16),
        tiles,
        tiles,
        pltpu.VMEM((SIDE, 1, LANES), F32),
        pltpu.VMEM((n_sp, 1, LANES), F32),
        tiles,
        tiles,
        pltpu.VMEM((n_tp, n_tp, own_rows, chunk), BF16),
        pltpu.VMEM((n_tp, n_tp - 1, own_rows, chunk), BF16),
        pltpu.VMEM((sent_rows, width), BF16),
        dma((11,)),
        dma((3,)),
        dma((6,)),
        dma((3,)),
        dma((3,)),
        dma((8,)),
        dma((3,)),
        dma((3,)),
        dma((n_tp + 1,)),
    ]
    result = pl.pallas_call(
        functools.partial(kernel, n_sp, n_tp, n_dp, heads),
        out_shape=pltpu.VMEM((own_rows, width), BF16),
        in_specs=[anywhere] * len(args),
        out_specs=vmem,
        scratch_shapes=scratch,
        compiler_params=pltpu.CompilerParams(
            collective_id=0, has_side_effects=True, vmem_limit_bytes=62_000_000
        ),
    )(*args)
    return result[None]


def solution(mesh):
    placed = (
        P("dp", ("sp", "tp"), None),
        P("dp", None),
        P("dp", "sp", None),
        P(),
        P(None, "sp", "tp"),
        P(),
        P("dp", "tp"),
        P("dp", "tp"),
        P("dp", "tp"),
        P("dp", "tp"),
        P(None, "dp", "tp"),
        P(None, "tp"),
        P(None, "tp"),
        P(None, "tp"),
        P(None, "tp"),
        P("tp"),
        P(("tp", "dp"), None),
    )
    return jax.shard_map(
        shards, mesh=mesh, in_specs=placed, out_specs=P("dp", ("sp", "tp"), None), check_vma=False
    )
```

```python
import functools

import jax
import jax.numpy as jnp
from jax import lax
from jax.experimental import pallas as pl
from jax.experimental.pallas import tpu as pltpu
from jax.sharding import PartitionSpec as P

STATE = 128
LANES = 128
PAD = 16
SIDE = 8
TILE = 16
EPSILON = 1e-06
MESH = pl.DeviceIdType.MESH
F32 = jnp.float32
BF16 = jnp.bfloat16


def silu(v):
    return v / (1.0 + jnp.exp(-v))


def softplus(v):
    return jnp.maximum(v, 0.0) + jnp.log1p(jnp.exp(-jnp.abs(v)))


def row_of(ref):
    return ref[...].astype(F32).reshape(1, ref.shape[0])


def dot(a, b, dims=((1,), (0,)), precision=None):
    return lax.dot_general(a, b, (dims, ((), ())), precision=precision, preferred_element_type=F32)


def reach(k):
    return min(k, SIDE - k)


def along():
    return sorted(range(1, SIDE), key=lambda k: -reach(k))


def far_first():
    steps = [(a, b) for a in range(SIDE) for b in range(SIDE) if a or b]
    return sorted(steps, key=lambda ab: -(reach(ab[0]) + reach(ab[1])))


def kernel(
    n_sp,
    n_tp,
    n_dp,
    heads,
    condition_in,
    source_in,
    gain_in,
    conv_x_in,
    conv_b_in,
    conv_c_in,
    rate_in,
    out_gain_in,
    latent,
    context,
    mod_weight,
    w_x,
    w_b,
    w_c,
    w_dt,
    w_z,
    w_out,
    out,
    condition,
    source,
    gain,
    conv_x,
    conv_b,
    conv_c,
    rate,
    out_gain,
    lat_all,
    ctx_buf,
    mod_buf,
    wx,
    wb,
    wc,
    wd,
    wz,
    wo,
    acts,
    edges,
    part,
    part_z,
    part_up,
    part_y,
    mods,
    halo,
    pre,
    hid,
    c_full,
    snd_c,
    rcv_c,
    snd_l,
    rcv_l,
    snd_t,
    rcv_t,
    snd_b,
    rcv_b,
    snd_o,
    rcv_o,
    weights_like,
    local_sem,
    weight_sem,
    pack_sem,
    line_send,
    line_recv,
    edge_sem,
    flat_send,
    flat_recv,
    o_sem,
):
    s = lax.axis_index("sp")
    t = lax.axis_index("tp")
    d = lax.axis_index("dp")
    z = s // SIDE
    y = lax.rem(s, SIDE)
    own_rows, width = latent.shape
    own_ctx = context.shape[0]
    ctx_rows = SIDE * own_ctx
    depth = mod_weight.shape[1]
    rows = n_tp * own_rows
    inner = w_x.shape[1]
    both = 2 * inner
    head_dim = inner // heads
    nh2 = 2 * heads
    up, down = lax.rem(s + 1, n_sp), lax.rem(s + n_sp - 1, n_sp)

    def remote(src, dst, send, recv, **to):
        return pltpu.make_async_remote_copy(
            src_ref=src, dst_ref=dst, send_sem=send, recv_sem=recv, device_id=to, device_id_type=MESH
        )

    local = []

    def fetch(src, dst):
        copy = pltpu.make_async_copy(src, dst, local_sem.at[len(local)])
        copy.start()
        local.append(copy)
        return copy

    early = [fetch(condition_in, condition), fetch(source_in, source), fetch(mod_weight, mod_buf)]
    barrier = pltpu.get_barrier_semaphore()

    def greet(**to):
        pl.semaphore_signal(barrier, inc=1, device_id=to, device_id_type=MESH)

    def on_z(k):
        return lax.rem(z + k, SIDE) * SIDE + y

    def on_y(k):
        return z * SIDE + lax.rem(y + k, SIDE)

    for k in along():
        greet(sp=on_z(k))
        greet(sp=on_y(k))
    for k in range(1, n_tp):
        greet(tp=lax.rem(t + k, n_tp))
    for k in range(1, n_dp):
        greet(dp=lax.rem(d + k, n_dp))
    z_up, z_down = lax.rem(z + 1, SIDE) * SIDE, lax.rem(z + SIDE - 1, SIDE) * SIDE
    is_first, is_last = s == 0, s == n_sp - 1

    @pl.when(jnp.logical_not(is_first))
    def _():
        greet(sp=down, tp=n_tp - 1)

    @pl.when(jnp.logical_not(is_last))
    def _():
        greet(sp=up, tp=0)


    def settle(ref, sem):
        pltpu.make_async_copy(ref, ref, sem).wait()

    lat_copy = fetch(latent, lat_all.at[t])
    ctx_copy = fetch(context, ctx_buf.at[y])
    small = [
        fetch(a, b)
        for a, b in (
            (gain_in, gain),
            (conv_x_in, conv_x),
            (conv_b_in, conv_b),
            (conv_c_in, conv_c),
            (rate_in, rate),
            (out_gain_in, out_gain),
        )
    ]
    pairs = ((w_x, wx), (w_b, wb), (w_dt, wd), (w_c, wc), (w_z, wz), (w_out, wo))
    places = []
    for src, dst in pairs:
        count = src.shape[0]
        places.append(dst.at[d] if src is w_dt else dst.at[pl.ds(d * count, count)])
        pltpu.make_async_copy(src, places[-1], weight_sem.at[0]).start()

    for copy in early:
        copy.wait()
    acts[0:1] = condition[...].astype(F32)
    acts[1:2] = row_of(source)
    per = LANES // depth
    block = acts[0:2, pl.ds(pl.multiple_of((s // per) * LANES, LANES), LANES)]
    active = jnp.concatenate([silu(block), jnp.zeros((PAD - 2, LANES), F32)], axis=0)
    own_acts = active[:, 0:depth]
    for j in range(1, per):
        own_acts = jnp.where(lax.rem(s, per) == j, active[:, j * depth : (j + 1) * depth], own_acts)
    own_acts = own_acts.astype(BF16)
    pieces = [dot(own_acts, mod_buf[k])[0:2] for k in range(mod_buf.shape[0])]
    cols = pieces[0].shape[1]

    def packed(rows_f32):
        low = [rows_f32[r : r + 1] - rows_f32[r : r + 1].astype(BF16).astype(F32) for r in (0, 2, 4)]
        return jnp.concatenate([rows_f32[0:5]] + low, axis=0).astype(BF16)

    def unpacked(total):
        fine = [total[r : r + 1] + total[5 + r // 2 : 6 + r // 2] for r in (0, 2, 4)]
        return jnp.concatenate(
            [fine[0], total[1:2], fine[1], total[3:4], fine[2], jnp.zeros((3, cols), F32)], axis=0
        )

    partial = jnp.concatenate(pieces + [jnp.zeros((2, cols), F32)], axis=0)
    part[...] = packed(partial)

    lat_copy.wait()
    edges[0] = lat_all[t, 0:1].astype(F32)
    edges[1] = lat_all[t, own_rows - 1 : own_rows].astype(F32)
    ctx_copy.wait()
    edges[2] = ctx_buf[y, 0:1].astype(F32)
    edges[3] = ctx_buf[y, own_ctx - 1 : own_ctx].astype(F32)

    expected = 2 * (SIDE - 1) + n_tp - 1 + n_dp - 1
    sends_up = (t == n_tp - 1) & jnp.logical_not(is_last)
    sends_down = (t == 0) & jnp.logical_not(is_first)
    ctx_sends_up = (y == SIDE - 1) & (z < SIDE - 1)
    ctx_sends_down = (y == 0) & (z > 0)
    expected = expected + jnp.where(sends_up, n_tp, 0) + jnp.where(sends_down, n_tp, 0)
    pl.semaphore_wait(barrier, expected)

    def line(src, dst, place, phase):
        for k in along():
            remote(src, dst.at[k - 1], line_send.at[phase], line_recv.at[phase], sp=place(k)).start()

    def line_wait(dst, phase):
        pltpu.make_async_copy(dst, dst, line_recv.at[phase]).wait()

    line(part, part_z, on_z, 0)
    for k in along():
        remote(ctx_buf.at[y], ctx_buf.at[y], pack_sem.at[2], pack_sem.at[3], sp=on_y(k)).start()
    for k in range(1, n_tp):
        remote(latent, lat_all.at[t], pack_sem.at[0], pack_sem.at[1], tp=lax.rem(t + k, n_tp)).start()
    ctx_up = [
        remote(edges.at[3], halo.at[2], edge_sem.at[0], edge_sem.at[6], sp=z_up + j) for j in range(SIDE)
    ]
    ctx_down = [
        remote(edges.at[2], halo.at[3], edge_sem.at[1], edge_sem.at[7], sp=z_down + j)
        for j in range(SIDE)
    ]
    lat_up = [
        remote(edges.at[1], halo.at[0], edge_sem.at[2], edge_sem.at[4], sp=up, tp=u)
        for u in range(n_tp)
    ]
    lat_down = [
        remote(edges.at[0], halo.at[1], edge_sem.at[3], edge_sem.at[5], sp=down, tp=u)
        for u in range(n_tp)
    ]

    @pl.when(sends_up)
    def _():
        for copy in lat_up:
            copy.start()

    @pl.when(sends_down)
    def _():
        for copy in lat_down:
            copy.start()

    for i, (src, dst) in enumerate(pairs):
        remote(src, places[i], weight_sem.at[1], weight_sem.at[2], dp=1 - d).start()

    def normed(v):
        return v * lax.rsqrt(jnp.mean(v * v, axis=1, keepdims=True) + EPSILON)

    line_wait(part_z, 0)
    others = part_z[0].astype(F32)
    for k in range(2, SIDE):
        others = others + part_z[k - 1].astype(F32)
    summed = partial + unpacked(others)
    part_up[...] = packed(summed)
    line(part_up, part_y, on_y, 1)

    @pl.when(ctx_sends_up)
    def _():
        for copy in ctx_up:
            copy.start()

    @pl.when(ctx_sends_down)
    def _():
        for copy in ctx_down:
            copy.start()


    line_wait(part_y, 1)
    others = part_y[0].astype(F32)
    for k in range(2, SIDE):
        others = others + part_y[k - 1].astype(F32)
    mods[t] = summed + unpacked(others)
    for k in range(1, n_tp):
        remote(mods.at[t], mods.at[t], pack_sem.at[4], pack_sem.at[5], tp=lax.rem(t + k, n_tp)).start()
    settle(lat_all.at[pl.ds(0, n_tp - 1)], pack_sem.at[1])
    for u in range(n_tp):
        pre[u * own_rows : (u + 1) * own_rows] = normed(lat_all[u].astype(F32))
    settle(ctx_buf.at[pl.ds(0, SIDE - 1)], pack_sem.at[3])
    for j in range(0, SIDE, 2):
        pre[rows + PAD + j * own_ctx : rows + PAD + (j + 2) * own_ctx] = normed(
            ctx_buf[j : j + 2].astype(F32).reshape(2 * own_ctx, width)
        )
    inner_edges = (jnp.logical_not(is_first), jnp.logical_not(is_last), z > 0, z < SIDE - 1)
    for j, inside_edge in enumerate(inner_edges):

        @pl.when(inside_edge)
        def _():
            settle(halo.at[j], edge_sem.at[4 + j])

        @pl.when(jnp.logical_not(inside_edge))
        def _():
            halo[j] = jnp.zeros((1, width), F32)

    pre[rows : rows + PAD] = normed(
        jnp.concatenate([halo[0], halo[1], halo[2], halo[3], jnp.zeros((PAD - 4, width), F32)], axis=0)
    )

    for copy in small:
        copy.wait()
    settle(mods.at[pl.ds(0, n_tp - 1)], pack_sem.at[5])

    def vector(row):
        return jnp.concatenate([mods[c][row : row + 1] for c in range(n_tp)], axis=1)

    gain_row = row_of(gain)
    lat_shift, ctx_shift = vector(0), vector(1)
    lat_gain = gain_row * (1.0 + vector(2))
    ctx_gain = gain_row * (1.0 + vector(3))
    for u in range(n_tp):
        cut = slice(u * own_rows, (u + 1) * own_rows)
        hid[cut] = (pre[cut] * lat_gain + lat_shift).astype(BF16)
    at_row = lax.broadcasted_iota(jnp.int32, (PAD, width), 0)
    edge = pre[rows : rows + PAD]
    hid[rows : rows + PAD] = jnp.where(
        at_row < 2, edge * lat_gain + lat_shift, edge * ctx_gain + ctx_shift
    ).astype(BF16)
    settle(weights_like, weight_sem.at[0])
    settle(weights_like, weight_sem.at[2])

    def shaped(values, before, after, taps, has_before=s > 0, has_after=s < n_sp - 1):
        count = values.shape[0]
        at = lax.broadcasted_iota(jnp.int32, values.shape, 0)
        before = jnp.where(has_before, before, 0.0)
        after = jnp.where(has_after, after, 0.0)
        earlier = jnp.where(at == 0, before, pltpu.roll(values, 1, 0))
        later = jnp.where(at == count - 1, after, pltpu.roll(values, count - 1, 0))
        w = taps[...].astype(F32)
        return silu(earlier * w[0:1] + values * w[1:2] + later * w[2:3]).astype(BF16)

    def project(weight, first, last):
        return dot(hid[first:last], weight[...]).astype(BF16).astype(F32)

    total = rows + PAD + ctx_rows
    half = wd.shape[3]
    spread_at = lax.broadcasted_iota(jnp.int32, (LANES, both), 0)
    spread_to = lax.broadcasted_iota(jnp.int32, (LANES, both), 1) // head_dim
    spreader = jnp.where((spread_to == spread_at) | (spread_to + nh2 == spread_at), 1.0, 0.0).astype(BF16)

    def expand(v):
        lane = lax.broadcasted_iota(jnp.int32, v.shape, 1)
        high = v.astype(BF16).astype(F32)
        low = pltpu.roll(v - high, nh2, 1)
        packed = jnp.where(lane < nh2, high, jnp.where(lane < 2 * nh2, low, 0.0))
        return dot(packed.astype(BF16), spreader)

    def running(steps):
        count = steps.shape[0]
        logs = -rates * steps
        high = logs.astype(BF16).astype(F32)
        rest = logs - high
        middle = rest.astype(BF16).astype(F32)
        low = rest - middle
        packed = high + pltpu.roll(middle, nh2, 1) + pltpu.roll(low, 2 * nh2, 1)
        a = lax.broadcasted_iota(jnp.int32, (2 * count, count), 0)
        b = lax.broadcasted_iota(jnp.int32, (2 * count, count), 1)
        keep = jnp.where(a < count, jnp.where(a >= b, 1.0, 0.0), jnp.where(a - count <= b, 1.0, 0.0))
        parts = dot(keep.astype(BF16), packed.astype(BF16))
        lane = lax.broadcasted_iota(jnp.int32, (count, LANES), 1)
        parts = jnp.where(lax.rem(lane, nh2) < heads, parts[0:count], parts[count:])
        sums = parts + pltpu.roll(parts, LANES - nh2, 1) + pltpu.roll(parts, LANES - 2 * nh2, 1)
        sums = jnp.where(lane < nh2, sums, 0.0)
        row_lane = lax.broadcasted_iota(jnp.int32, (1, LANES), 1)
        ends = jnp.where(row_lane < heads, sums[count - 1 : count], sums[0:1])
        return sums, ends

    def moved(values, steps):
        wide = jnp.concatenate([values, values], axis=1)
        return (wide * expand(steps)).astype(BF16)

    def spread_out(src, dst, phase):
        for a, b in far_first():
            to = lax.rem(z + a, SIDE) * SIDE + lax.rem(y + b, SIDE)
            remote(src.at[to], dst.at[s], flat_send.at[phase], flat_recv.at[phase], sp=to).start()
        dst[s] = src[s]

    def all_in(dst, phase):
        most = dst.at[pl.ds(0, n_sp - 1)]
        pltpu.make_async_copy(most, most, flat_recv.at[phase]).wait()

    def tiles(dst, state):
        for a in range(SIDE):
            for b in range(SIDE):
                dst[a * SIDE + b] = state[
                    b * TILE : (b + 1) * TILE, a * LANES : (a + 1) * LANES
                ].astype(BF16)

    dt_taps = [
        jnp.concatenate(
            [wd[r, 0].astype(F32), wd[r, 1].astype(F32), jnp.zeros((LANES - nh2, half), F32)], axis=0
        ).astype(BF16)
        for r in range(n_dp)
    ]

    def steps_of(first, last):
        features = None
        for r in range(n_dp):
            one = dot(hid[first:last, r * half : (r + 1) * half], dt_taps[r], ((1,), (1,)))
            features = one if features is None else features + one
        return softplus(features.astype(BF16).astype(F32))

    rates = jnp.concatenate([rate[0:1], rate[1:2], jnp.zeros((1, LANES - nh2), F32)], axis=1)
    l_steps = steps_of(0, rows)
    l_sums, l_ends = running(l_steps)
    ends = expand(jnp.exp(jnp.broadcast_to(l_ends, (8, LANES))))
    for a in range(SIDE):
        snd_t[a] = ends[0:1, a * LANES : (a + 1) * LANES]
    px = project(wx, 0, rows + PAD)
    pb = project(wb, 0, rows + PAD)
    x_in = shaped(px[0:rows], px[rows : rows + 1], px[rows + 1 : rows + 2], conv_x).astype(F32)
    b_in = shaped(pb[0:rows], pb[rows : rows + 1], pb[rows + 1 : rows + 2], conv_b)
    l_moved = moved(x_in, l_steps)
    l_scaled = (l_moved.astype(F32) * expand(jnp.exp(l_ends - l_sums))).astype(BF16)
    tiles(snd_l, dot(b_in, l_scaled, ((0,), (0,))))
    spread_out(snd_l, rcv_l, 0)
    for a, b in far_first():
        row = lax.rem(z + a, SIDE)
        to = row * SIDE + lax.rem(y + b, SIDE)
        remote(snd_t.at[row], rcv_t.at[s], flat_send.at[2], flat_recv.at[2], sp=to).start()
    rcv_t[s] = snd_t[z]

    hid[rows + PAD : rows + PAD + ctx_rows] = (
        pre[rows + PAD : rows + PAD + ctx_rows] * ctx_gain + ctx_shift
    ).astype(BF16)
    c_steps = steps_of(rows + PAD, total)
    c_sums, c_ends = running(c_steps)
    c_decay = expand(jnp.exp(jnp.broadcast_to(c_ends, (8, LANES))))
    cpx = project(wx, rows, total)
    cpb = project(wb, rows, total)
    c_edges = (z > 0, z < SIDE - 1)
    cx_in = shaped(cpx[PAD:], cpx[2:3], cpx[3:4], conv_x, *c_edges).astype(F32)
    cb_in = shaped(cpb[PAD:], cpb[2:3], cpb[3:4], conv_b, *c_edges)
    c_moved = moved(cx_in, c_steps)
    c_scaled = (c_moved.astype(F32) * expand(jnp.exp(c_ends - c_sums))).astype(BF16)
    c_full[...] = dot(cb_in, c_scaled, ((0,), (0,)))
    c_rows = c_full[pl.ds(pl.multiple_of(y * TILE, TILE), TILE)]
    c_high = c_decay.astype(BF16).astype(F32)
    c_tail = jnp.where(lax.broadcasted_iota(jnp.int32, c_decay.shape, 0) == 0, c_high, c_decay - c_high)
    c_all = jnp.concatenate([c_rows, c_tail], axis=0).astype(BF16)
    for a in range(SIDE):
        snd_c[a] = c_all[:, a * LANES : (a + 1) * LANES]
    for k in along():
        to = lax.rem(z + k, SIDE)
        remote(snd_c.at[to], rcv_c.at[z], line_send.at[2], line_recv.at[2], sp=on_z(k)).start()
    rcv_c[z] = snd_c[z]

    pc = project(wc, 0, rows + PAD)
    c_in = shaped(pc[0:rows], pc[rows : rows + 1], pc[rows + 1 : rows + 2], conv_c)
    scores = dot(c_in, b_in, ((1,), (1,)))
    at_t = lax.broadcasted_iota(jnp.int32, (rows, rows), 0)
    at_s = lax.broadcasted_iota(jnp.int32, (rows, rows), 1)
    sums_t = jnp.transpose(l_sums)

    def weights(lane, keep):
        gap = l_sums[:, lane : lane + 1] - sums_t[lane : lane + 1]
        return jnp.where(keep, scores * jnp.exp(jnp.minimum(gap, 0.0)), 0.0).astype(BF16)

    pair = LANES // head_dim
    inside = []
    lane_head = lax.broadcasted_iota(jnp.int32, (rows, LANES), 1) // head_dim
    for p in range(heads // pair):
        cut = slice(p * LANES, (p + 1) * LANES)
        cut_b = slice(inner + p * LANES, inner + (p + 1) * LANES)
        sources = jnp.concatenate([l_moved[:, cut], l_moved[:, cut_b]], axis=0)
        value = None
        for i in range(pair):
            h = p * pair + i
            w = jnp.concatenate([weights(h, at_t >= at_s), weights(heads + h, at_t <= at_s)], axis=1)
            one = dot(w, sources)
            value = one if value is None else jnp.where(lane_head == i, one, value)
        inside.append(value)
    inside = jnp.concatenate(inside, axis=1)
    growth = expand(jnp.exp(l_sums))
    gate = silu(project(wz, 0, rows))
    inside = inside * gate
    growth = growth * jnp.concatenate([gate, gate], axis=1)

    forward = z < SIDE // 2

    def place(j, count=n_sp):
        return jnp.where(forward, j, count - 1 - j)

    line_wait(rcv_c.at[pl.ds(0, SIDE - 1)], 2)
    state = jnp.zeros((TILE, LANES), F32)
    for j in range(SIDE):
        i = place(j, SIDE)
        piece = rcv_c[i].astype(F32)
        state = state * (piece[TILE : TILE + 1] + piece[TILE + 1 : TILE + 2]) + piece[0:TILE]
    all_in(rcv_t, 2)
    all_in(rcv_l, 0)

    def latent_step(j, state):
        i = place(j)
        snd_b[i] = state.astype(BF16)
        return state * rcv_t[i] + rcv_l[i].astype(F32)

    lax.fori_loop(0, n_sp, latent_step, state, unroll=8)
    for row in range(SIDE):
        for b in along():
            to = row * SIDE + lax.rem(y + b, SIDE)
            remote(snd_b.at[to], rcv_b.at[s], flat_send.at[1], flat_recv.at[1], sp=to).start()

        @pl.when(z != row)
        def _():
            to = row * SIDE + y
            remote(snd_b.at[to], rcv_b.at[s], flat_send.at[1], flat_recv.at[1], sp=to).start()

    rcv_b[s] = snd_b[s]
    all_in(rcv_b, 1)
    entering = jnp.concatenate(
        [rcv_b[a * SIDE : (a + 1) * SIDE].reshape(STATE, LANES) for a in range(SIDE)], axis=1
    )
    carried = dot(c_in, entering) * growth
    gated = inside + carried[:, 0:inner] + carried[:, inner:both]
    ny = (
        gated
        * lax.rsqrt(jnp.mean(gated * gated, axis=1, keepdims=True) + EPSILON)
        * row_of(out_gain)
    ).astype(BF16)

    chunks = n_tp
    chunk = width // chunks
    far_tp = sorted(range(1, n_tp), key=lambda k: -min(k, n_tp - k))
    for c in range(chunks):
        cut = slice(c * chunk, (c + 1) * chunk)
        result = dot(ny, wo[:, cut]).astype(BF16)
        for u in range(n_tp):
            snd_o[c, u] = result[u * own_rows : (u + 1) * own_rows]
        for k in far_tp:
            to = lax.rem(t + k, n_tp)
            remote(snd_o.at[c, to], rcv_o.at[c, k - 1], o_sem.at[chunks], o_sem.at[c], tp=to).start()

    most = pl.ds(0, SIDE - 1)
    for phase, sent in enumerate((part_z, part_y, rcv_c.at[most])):
        settle(sent, line_send.at[phase])
    for phase, sent in enumerate((rcv_l, rcv_b, rcv_t)):
        settle(sent.at[pl.ds(0, n_sp - 1)], flat_send.at[phase])
    settle(weights_like, weight_sem.at[1])
    settle(lat_all.at[pl.ds(0, n_tp - 1)], pack_sem.at[0])
    settle(ctx_buf.at[pl.ds(0, SIDE - 1)], pack_sem.at[2])
    settle(mods.at[pl.ds(0, n_tp - 1)], pack_sem.at[4])

    for j, (ref, sends) in enumerate(
        ((acts, ctx_sends_up), (acts, ctx_sends_down), (halo, sends_up), (halo, sends_down))
    ):

        @pl.when(sends)
        def _():
            settle(ref, edge_sem.at[j])


    for c in range(chunks):
        mixed = snd_o[c, t].astype(F32)
        settle(rcv_o.at[c], o_sem.at[c])
        for k in range(1, n_tp):
            mixed = mixed + rcv_o[c, k - 1].astype(F32)
        out[:, c * chunk : (c + 1) * chunk] = (mods[c][4:5] * mixed).astype(BF16)
    settle(rcv_o, o_sem.at[chunks])


def shards(
    latent,
    condition,
    context,
    context_source,
    mod_weight,
    norm_gain,
    w_x,
    w_b,
    w_c,
    w_z,
    w_dt,
    conv_x,
    conv_b,
    conv_c,
    decay_rate,
    out_gain,
    w_out,
):
    n_sp, n_tp, n_dp = lax.axis_size("sp"), lax.axis_size("tp"), lax.axis_size("dp")
    assert n_sp == SIDE * SIDE
    own_rows, width = latent.shape[1:]
    own_ctx = context.shape[1]
    ctx_rows = SIDE * own_ctx
    cols = mod_weight.shape[2]
    inner = w_x.shape[1]
    heads = decay_rate.shape[1]
    assert STATE == SIDE * TILE and 2 * inner == SIDE * LANES
    rows = n_tp * own_rows
    total = rows + PAD + ctx_rows
    chunk = width // n_tp
    vmem = pl.BlockSpec(memory_space=pltpu.VMEM)
    anywhere = pl.BlockSpec(memory_space=pl.ANY)
    dma = pltpu.SemaphoreType.DMA
    args = (
        condition,
        context_source,
        norm_gain,
        conv_x,
        conv_b,
        conv_c,
        decay_rate,
        out_gain,
        latent[0],
        context[0],
        mod_weight,
        w_x,
        w_b,
        w_c,
        jnp.swapaxes(w_dt, 1, 2),
        w_z,
        w_out,
    )
    tiles = pltpu.VMEM((n_sp, TILE, LANES), BF16)
    sent_rows = sum(w.size for w in (w_x, w_b, w_c, w_dt, w_z, w_out)) // width
    scratch = [pltpu.VMEM(a.shape, a.dtype) for a in args[:8]] + [
        pltpu.VMEM((n_tp, own_rows, width), BF16),
        pltpu.VMEM((SIDE, own_ctx, width), BF16),
        pltpu.VMEM(mod_weight.shape, BF16),
        pltpu.VMEM((w_x.shape[0] * n_dp, inner), BF16),
        pltpu.VMEM((w_b.shape[0] * n_dp, w_b.shape[1]), BF16),
        pltpu.VMEM((w_c.shape[0] * n_dp, w_c.shape[1]), BF16),
        pltpu.VMEM((n_dp, 2, heads, w_dt.shape[1]), BF16),
        pltpu.VMEM((w_z.shape[0] * n_dp, inner), BF16),
        pltpu.VMEM((w_out.shape[0] * n_dp, width), BF16),
        pltpu.VMEM((8, width), F32),
        pltpu.VMEM((4, 1, width), F32),
        pltpu.VMEM((8, cols), BF16),
        pltpu.VMEM((SIDE - 1, 8, cols), BF16),
        pltpu.VMEM((8, cols), BF16),
        pltpu.VMEM((SIDE - 1, 8, cols), BF16),
        pltpu.VMEM((n_tp, 8, cols), F32),
        pltpu.VMEM((4, 1, width), F32),
        pltpu.VMEM((total, width), F32),
        pltpu.VMEM((total, width), BF16),
        pltpu.VMEM((STATE, 2 * inner), F32),
        pltpu.VMEM((SIDE, TILE + 8, LANES), BF16),
        pltpu.VMEM((SIDE, TILE + 8, LANES), BF16),
        tiles,
        tiles,
        pltpu.VMEM((SIDE, 1, LANES), F32),
        pltpu.VMEM((n_sp, 1, LANES), F32),
        tiles,
        tiles,
        pltpu.VMEM((n_tp, n_tp, own_rows, chunk), BF16),
        pltpu.VMEM((n_tp, n_tp - 1, own_rows, chunk), BF16),
        pltpu.VMEM((sent_rows, width), BF16),
        dma((11,)),
        dma((3,)),
        dma((6,)),
        dma((3,)),
        dma((3,)),
        dma((8,)),
        dma((3,)),
        dma((3,)),
        dma((n_tp + 1,)),
    ]
    result = pl.pallas_call(
        functools.partial(kernel, n_sp, n_tp, n_dp, heads),
        out_shape=pltpu.VMEM((own_rows, width), BF16),
        in_specs=[anywhere] * len(args),
        out_specs=vmem,
        scratch_shapes=scratch,
        compiler_params=pltpu.CompilerParams(
            collective_id=0, has_side_effects=True, vmem_limit_bytes=62_000_000
        ),
    )(*args)
    return result[None]


def solution(mesh):
    placed = (
        P("dp", ("sp", "tp"), None),
        P("dp", None),
        P("dp", "sp", None),
        P(),
        P(None, "sp", "tp"),
        P(),
        P("dp", "tp"),
        P("dp", "tp"),
        P("dp", "tp"),
        P("dp", "tp"),
        P(None, "dp", "tp"),
        P(None, "tp"),
        P(None, "tp"),
        P(None, "tp"),
        P(None, "tp"),
        P("tp"),
        P(("tp", "dp"), None),
    )
    return jax.shard_map(
        shards, mesh=mesh, in_specs=placed, out_specs=P("dp", ("sp", "tp"), None), check_vma=False
    )
```
